256 devices in a mesh: kv: 32 (over z, y), tp: 8 (over x, core).
Axes of the slice: x: 4, y: 4, z: 8, core: 2. Of those that a mesh axis runs over, the one named last changes fastest.
Arguments:
- tokens: bfloat16 [16, 4, 4096], P(None, None, 'kv'), may hold values from -20 to 20
- mix_gain: float32 [4096], P('kv'), may hold values from 0.1 to 1.9
- w_query: bfloat16 [4096, 2048], P('kv', 'tp'), may hold values from -0.09375 to 0.09375
- w_key: bfloat16 [4096, 2048], P('kv', 'tp'), may hold values from -0.09375 to 0.09375
- w_value: bfloat16 [4096, 2048], P('kv', 'tp'), may hold values from -0.09375 to 0.09375
- w_forget: bfloat16 [4096, 16], replicated, may hold values from -0.09375 to 0.09375
- forget_bias: float32 [16], P('tp'), may hold values from -1 to 3
- key_cache: bfloat16 [16, 16384, 2048], P(None, 'kv', 'tp'), may hold values from -6 to 6
- value_cache: bfloat16 [16, 16384, 2048], P(None, 'kv', 'tp'), may hold values from -6 to 6
- cum_gate: float32 [16, 16, 16384], P(None, 'tp', 'kv'), may hold values from -2236.08 to 0, as said below
- lengths: int32 [16], replicated, may hold values from 1 to 16384, 65524 in all
- w_out: bfloat16 [2048, 4096], P('tp', 'kv'), may hold values from -0.125 to 0.125
- mlp_gain: float32 [4096], P('kv'), may hold values from 0.1 to 1.9
- w_gate: bfloat16 [4096, 11264], P('kv', 'tp'), may hold values from -0.09375 to 0.09375
- w_up: bfloat16 [4096, 11264], P('kv', 'tp'), may hold values from -0.09375 to 0.09375
- w_down: bfloat16 [11264, 4096], P('tp', 'kv'), may hold values from -0.0546875 to 0.0546875
Outputs:
- result: bfloat16 [16, 4, 4096], P(None, None, 'kv')
The draws below stay inside these ranges and needn't reach their ends.
Inputs may be any that keep to these rules, and one draw needn't show every extreme that they name: `cum_gate`: never rising along positions. `lengths`: one sequence fills all 16384 positions.
All inputs are finite; a program needn't handle non-finite values.
Results may differ from the reference program's by a relative error of at most 0.02.
Values may be sent and summed in bfloat16 or wider, within the bound.
A program may use at most 64 MiB of HBM per device.

```python
import math
import jax
import jax.numpy as jnp
import numpy as np
from jax import lax

D = 4096
ATTENTION_HEADS = 16
HEAD_DIM = 128
FF = 11264
NEW = 4
SEQUENCE_COUNT = 16
POS_DEV = 512
CACHE_SLOTS = 16384
N_KV = 32
N_TP = 8


def draw_tokens(key, part):
    base_key, scale_key = jax.random.split(jax.random.fold_in(key, 11))
    values = jax.random.normal(base_key, (SEQUENCE_COUNT, NEW, D), jnp.float32)
    column = jnp.arange(D, dtype=jnp.float32) / D
    jaggedness = jax.random.uniform(scale_key, (D,), jnp.float32, 0.6, 1.4)
    col_scale = 3.0 ** column * jaggedness * 0.6
    return jnp.clip(values * col_scale, -20.0, 20.0).astype(jnp.bfloat16)


def draw_cum_gate(key, part):
    random_subkeys = jax.random.split(jax.random.fold_in(key, 23), 8)
    head_order = jax.random.permutation(random_subkeys[0], ATTENTION_HEADS)
    sluggish_heads = head_order >= ATTENTION_HEADS // 2
    fast_rate = jax.random.uniform(random_subkeys[1], (SEQUENCE_COUNT, ATTENTION_HEADS, 1), jnp.float32, 1.0 / 60.0, 1.0 / 30.0)
    slow_rate = jax.random.uniform(random_subkeys[2], (SEQUENCE_COUNT, ATTENTION_HEADS, 1), jnp.float32, 0.5, 1.5) / CACHE_SLOTS
    forget_speed = jnp.where(sluggish_heads[None, :, None], slow_rate, fast_rate)
    block_count = CACHE_SLOTS // POS_DEV
    block_multiplier = jnp.exp(jax.random.uniform(random_subkeys[3], (SEQUENCE_COUNT, ATTENTION_HEADS, block_count, 1), jnp.float32, -0.7, 0.7))
    block_multiplier = jnp.broadcast_to(block_multiplier, (SEQUENCE_COUNT, ATTENTION_HEADS, block_count, POS_DEV)).reshape(SEQUENCE_COUNT, ATTENTION_HEADS, CACHE_SLOTS)
    jaggedness = jax.random.uniform(random_subkeys[4], (SEQUENCE_COUNT, ATTENTION_HEADS, CACHE_SLOTS), jnp.float32, 0.3, 1.7)
    sudden_mask = jax.random.uniform(random_subkeys[5], (SEQUENCE_COUNT, ATTENTION_HEADS, CACHE_SLOTS), jnp.float32) < 4.0 / CACHE_SLOTS
    sudden_dropout = jax.random.uniform(random_subkeys[6], (SEQUENCE_COUNT, ATTENTION_HEADS, CACHE_SLOTS), jnp.float32, 0.22, 0.69)
    sudden_dropout = jnp.where(sudden_mask & sluggish_heads[None, :, None], sudden_dropout, 0.0)
    history_start = -jax.random.uniform(random_subkeys[7], (SEQUENCE_COUNT, ATTENTION_HEADS, 1), jnp.float32, 20.0, 260.0)
    gate_logarithms = -forget_speed * block_multiplier * jaggedness - sudden_dropout
    return (history_start + jnp.cumsum(gate_logarithms, axis=2)).astype(jnp.float32)


def block_scale(own_key, dims, cuts, low, largest):
    def one(dim, shards_of):
        heights = jax.random.uniform(jax.random.fold_in(jax.random.fold_in(own_key, 6), dim), (shards_of,), jnp.float32, low / len(cuts), largest / len(cuts))
        return jnp.repeat(jnp.exp(heights), dims[dim] // shards_of).reshape((-1,) + (1,) * (len(dims) - dim - 1))

    gain = one(*cuts[0])
    for cut in cuts[1:]:
        gain = gain * one(*cut)
    return gain


def profile(amount, total, bound, skew):
    loads = [(1 << 20) // math.isqrt(standing ** skew) + 1 for standing in range(2, amount + 1)]
    surplus, given = total - bound - (amount - 1), [1] * (amount - 1)
    while surplus > 0:
        candidates = [i for i in range(amount - 1) if given[i] < bound]
        pool, budget = sum([loads[i] for i in candidates]), surplus
        for i in candidates:
            addition = min(bound - given[i], max(1, budget * loads[i] // pool), surplus)
            given[i] = given[i] + addition
            surplus = surplus - addition
    return np.array([bound] + given)


def uneven(rng, count, total, reach, lean):
    if count == 2:
        one = jax.random.randint(rng, (), max(1, total - reach), min(reach, total - 1) + 1)
        return jnp.stack([one, total - one])
    sizes = jnp.asarray(profile(count, total, reach, lean), jnp.int32)
    pairs = (count - 1) // 2
    source_of, taker = sizes[1:1 + 2 * pairs:2], sizes[2:2 + 2 * pairs:2]
    slack = jnp.minimum(source_of - 1, reach - taker)
    passed = jax.random.randint(jax.random.fold_in(rng, 1), (pairs,), 0, 1 << 20) % (slack + 1)
    sizes = sizes.at[1:1 + 2 * pairs:2].set(source_of - passed).at[2:2 + 2 * pairs:2].set(taker + passed)
    return sizes[jax.random.permutation(jax.random.fold_in(rng, 2), count)]


def gaussian(rng, shape, deviation, bound, cuts=(), kind=jnp.bfloat16):
    array = deviation * jax.random.normal(rng, shape, jnp.float32)
    if cuts:
        array = array * block_scale(rng, shape, cuts, -0.22, 0.18)
    return jnp.clip(array, -bound, bound).astype(kind)


def setup_inputs(seed: int = 0) -> dict:
    key_of = jax.random.split(jax.random.key(seed), 17)
    tokens = draw_tokens(jax.random.fold_in(key_of[16], 71), 0)
    mix_gain = jnp.clip(1.0 + 0.18 * jax.random.normal(key_of[1], (D,), jnp.float32), 0.1, 1.9)
    w_query = gaussian(key_of[2], (D, ATTENTION_HEADS * HEAD_DIM), D ** -0.5, 0.09375, ((0, 32), (1, 8)))
    w_key = gaussian(key_of[3], (D, ATTENTION_HEADS * HEAD_DIM), D ** -0.5, 0.09375, ((0, 32), (1, 8)))
    w_value = gaussian(key_of[4], (D, ATTENTION_HEADS * HEAD_DIM), D ** -0.5, 0.09375, ((0, 32), (1, 8)))
    w_forget = gaussian(key_of[5], (D, ATTENTION_HEADS), D ** -0.5, 0.09375)
    forget_bias = jnp.clip(-1.0 + 4.0 * jax.random.uniform(key_of[6], (ATTENTION_HEADS,), jnp.float32) ** block_scale(key_of[6], (ATTENTION_HEADS,), ((0, 8),), -0.2, 0.2), -1.0, 3.0)
    key_cache = gaussian(key_of[7], (SEQUENCE_COUNT, CACHE_SLOTS, ATTENTION_HEADS * HEAD_DIM), 1.0, 6.0, ((1, 32), (2, 8)))
    value_cache = gaussian(key_of[8], (SEQUENCE_COUNT, CACHE_SLOTS, ATTENTION_HEADS * HEAD_DIM), 1.0, 6.0, ((1, 32), (2, 8)))
    cum_gate = draw_cum_gate(jax.random.fold_in(key_of[16], 71), 0)
    lengths = uneven(key_of[10], SEQUENCE_COUNT, CACHE_SLOTS + (SEQUENCE_COUNT - 1) * (CACHE_SLOTS // 5), CACHE_SLOTS, 2).astype(jnp.int32)
    w_out = gaussian(key_of[11], (ATTENTION_HEADS * HEAD_DIM, D), (ATTENTION_HEADS * HEAD_DIM) ** -0.5, 0.125, ((0, 8), (1, 32)))
    mlp_gain = jnp.clip(1.0 + 0.18 * jax.random.normal(key_of[12], (D,), jnp.float32), 0.1, 1.9)
    w_gate = gaussian(key_of[13], (D, FF), D ** -0.5, 0.09375, ((0, 32), (1, 8)))
    w_up = gaussian(key_of[14], (D, FF), D ** -0.5, 0.09375, ((0, 32), (1, 8)))
    w_down = gaussian(key_of[15], (FF, D), FF ** -0.5, 0.0546875, ((0, 8), (1, 32)))
    return dict(tokens=tokens, mix_gain=mix_gain, w_query=w_query, w_key=w_key, w_value=w_value, w_forget=w_forget, forget_bias=forget_bias, key_cache=key_cache, value_cache=value_cache, cum_gate=cum_gate, lengths=lengths, w_out=w_out, mlp_gain=mlp_gain, w_gate=w_gate, w_up=w_up, w_down=w_down)


EPSILON = 1e-06
NEG_FILL = -1e+30

def widen(values):
    return lax.optimization_barrier(values).astype(jnp.float32)

def grouped_sum(left, weight, group_width):
    summed = jnp.zeros((left.shape[0], weight.shape[1]), jnp.float32)
    for group in range(N_TP):
        partial_product = jnp.dot(left[:, group * group_width:(group + 1) * group_width], weight[group * group_width:(group + 1) * group_width], preferred_element_type=jnp.float32)
        summed = summed + widen(partial_product.astype(jnp.bfloat16))
    return summed

def reference(tokens, mix_gain, w_query, w_key, w_value, w_forget, forget_bias, key_cache, value_cache, cum_gate, lengths, w_out, mlp_gain, w_gate, w_up, w_down):
    row_count = SEQUENCE_COUNT * NEW
    inputs = tokens.reshape(row_count, D).astype(jnp.float32)
    inv_norm = lax.rsqrt(lax.optimization_barrier(jnp.sum(inputs * inputs, axis=1)) / D + EPSILON)[:, None]
    scaled = (inputs * mix_gain).astype(jnp.bfloat16)

    def project(weight):
        return inv_norm * jnp.dot(scaled, weight, preferred_element_type=jnp.float32)
    query = project(w_query).astype(jnp.bfloat16).reshape(SEQUENCE_COUNT, NEW, ATTENTION_HEADS, HEAD_DIM)
    key_new = project(w_key).astype(jnp.bfloat16).reshape(SEQUENCE_COUNT, NEW, ATTENTION_HEADS, HEAD_DIM)
    value_new = project(w_value).astype(jnp.bfloat16).reshape(SEQUENCE_COUNT, NEW, ATTENTION_HEADS, HEAD_DIM)
    log_forget = jax.nn.log_sigmoid(project(w_forget) + forget_bias).reshape(SEQUENCE_COUNT, NEW, ATTENTION_HEADS)
    score_scale = HEAD_DIM ** (-0.5)
    query_wide = widen(query)

    def past_block(block_index):
        offset = block_index * POS_DEV
        cached_keys = lax.dynamic_slice_in_dim(key_cache, offset, POS_DEV, 1).astype(jnp.float32)
        cached_keys = cached_keys.reshape(SEQUENCE_COUNT, POS_DEV, ATTENTION_HEADS, HEAD_DIM)
        cached_values = lax.dynamic_slice_in_dim(value_cache, offset, POS_DEV, 1).astype(jnp.float32)
        cached_values = cached_values.reshape(SEQUENCE_COUNT, POS_DEV, ATTENTION_HEADS, HEAD_DIM)
        cum_block = lax.dynamic_slice_in_dim(cum_gate, offset, POS_DEV, 2)
        scores = jnp.einsum('bthd,bphd->bthp', query_wide, cached_keys) * score_scale - cum_block[:, None]
        positions = offset + jnp.arange(POS_DEV, dtype=jnp.int32)
        live_mask = (positions[None, :] < lengths[:, None])[:, None, None, :]
        scores = jnp.where(live_mask, scores, NEG_FILL)
        block_peak = lax.optimization_barrier(jnp.max(scores, axis=3))
        weights = jnp.where(live_mask, jnp.exp(scores - block_peak[..., None]), 0.0)
        block_total = lax.optimization_barrier(jnp.sum(weights, axis=3))
        block_sum = jnp.einsum('bthp,bphd->bthd', widen(weights.astype(jnp.bfloat16)), cached_values)
        return (block_peak, block_total, block_sum)
    peaks, totals, sums = lax.map(past_block, jnp.arange(N_KV, dtype=jnp.int32))
    past_peak = lax.optimization_barrier(jnp.max(peaks, axis=0))
    factors = jnp.exp(peaks - past_peak)
    past_total = lax.optimization_barrier(jnp.sum(totals * factors, axis=0))
    past_sum = lax.optimization_barrier(jnp.sum(sums * factors[..., None], axis=0))
    last_index = jnp.broadcast_to((lengths - 1).astype(jnp.int32)[:, None, None], (SEQUENCE_COUNT, ATTENTION_HEADS, 1))
    last_cum = jnp.take_along_axis(cum_gate, last_index, axis=2)[..., 0]
    key_cum = last_cum[:, None, :] + jnp.cumsum(log_forget, axis=1)
    own_scores = jnp.einsum('bthd,bshd->bths', query_wide, widen(key_new)) * score_scale
    own_scores = own_scores - jnp.transpose(key_cum, (0, 2, 1))[:, None]
    causal = (jnp.arange(NEW)[:, None] >= jnp.arange(NEW)[None, :])[None, :, None, :]
    own_scores = jnp.where(causal, own_scores, NEG_FILL)
    peak_score = jnp.maximum(past_peak, lax.optimization_barrier(jnp.max(own_scores, axis=3)))
    past_factor = jnp.exp(past_peak - peak_score)
    own_weights = jnp.where(causal, jnp.exp(own_scores - peak_score[..., None]), 0.0)
    numerator = past_sum * past_factor[..., None] + jnp.einsum('bths,bshd->bthd', widen(own_weights.astype(jnp.bfloat16)), widen(value_new))
    denominator = past_total * past_factor + lax.optimization_barrier(jnp.sum(own_weights, axis=3))
    attended = (numerator / denominator[..., None]).astype(jnp.bfloat16).reshape(row_count, ATTENTION_HEADS * HEAD_DIM)
    attn_out = grouped_sum(attended, w_out, ATTENTION_HEADS // N_TP * HEAD_DIM)
    middle = (inputs + attn_out).astype(jnp.bfloat16)
    middle_wide = middle.astype(jnp.float32)
    inv_norm2 = lax.rsqrt(lax.optimization_barrier(jnp.sum(middle_wide * middle_wide, axis=1)) / D + EPSILON)[:, None]
    scaled2 = (middle_wide * mlp_gain).astype(jnp.bfloat16)
    gate = inv_norm2 * jnp.dot(scaled2, w_gate, preferred_element_type=jnp.float32)
    up_proj = inv_norm2 * jnp.dot(scaled2, w_up, preferred_element_type=jnp.float32)
    hidden = (jax.nn.silu(gate) * up_proj).astype(jnp.bfloat16)
    mixed = grouped_sum(hidden, w_down, FF // N_TP)
    return (middle_wide + mixed).astype(jnp.bfloat16).reshape(SEQUENCE_COUNT, NEW, D)
```

```python
import jax
import jax.numpy as jnp
from jax import lax
from jax.experimental import pallas as pl
from jax.experimental.pallas import tpu as pltpu
from jax.sharding import PartitionSpec as P

D = 4096
EPSILON = 1e-06
NEG_FILL = -1e30
SEQS = 16
NEW = 4
ROWS = SEQS * NEW
HEADS = 2
HD = 128
WIDTH = 128
POS = 512
FF = 1408
HALF = 768
SHIFT = FF - HALF
KV = 32
TP = 8
ZS, YS = 8, 4
F32 = jnp.float32
BF16 = jnp.bfloat16
MESH = pl.DeviceIdType.MESH


def far_first(count):
    return sorted(range(1, count), key=lambda d: -min(d, count - d))


OFFSETS = sorted(
    ((dz, dy) for dz in range(ZS) for dy in range(YS) if dz or dy),
    key=lambda o: -(min(o[0], ZS - o[0]) + min(o[1], YS - o[1])),
)


def kernel(
    lengths_ref,
    bias_ref,
    tokens_hbm,
    mix_hbm,
    wq_hbm,
    wk_hbm,
    wv_hbm,
    wf_hbm,
    kc_hbm,
    vc_hbm,
    cg_hbm,
    wo_hbm,
    mlp_hbm,
    wg_hbm,
    wu_hbm,
    wd_hbm,
    out_ref,
    tok,
    mix,
    wq,
    wk,
    wv,
    wf,
    kc,
    vc,
    cg,
    wo,
    mlp,
    wg,
    wu,
    wd,
    xs,
    est,
    qblk,
    att,
    hid,
    send_a,
    recv_a,
    send_q,
    recv_q,
    send_b,
    recv_b,
    send_t,
    recv_t,
    send_c,
    recv_c,
    send_e,
    recv_e,
    send_h,
    recv_h,
    send_f,
    recv_f,
    in_sem,
    send_sem,
    recv_sem,
):
    k = lax.axis_index("kv")
    t = lax.axis_index("tp")
    z, y = k // YS, lax.rem(k, YS)
    head = lax.rem(k, 2)
    mine = k // 2

    loads = {}
    sources = dict(
        tok=(tokens_hbm, tok),
        mix=(mix_hbm, mix),
        wq=(wq_hbm, wq),
        wk=(wk_hbm, wk),
        wv=(wv_hbm, wv),
        wf=(wf_hbm.at[pl.ds(pl.multiple_of(k * WIDTH, WIDTH), WIDTH)], wf),
        kc=(kc_hbm, kc),
        vc=(vc_hbm, vc),
        cg=(cg_hbm, cg),
        wo=(wo_hbm, wo),
        mlp=(mlp_hbm, mlp),
        wg=(wg_hbm, wg),
        wu=(wu_hbm, wu),
        wd=(wd_hbm, wd),
    )
    for n, (name, (src, dst)) in enumerate(sources.items()):
        loads[name] = pltpu.make_async_copy(src, dst, in_sem.at[n])
        loads[name].start()

    kv_peers = [lax.rem(z + dz, ZS) * YS + lax.rem(y + dy, YS) for dz, dy in OFFSETS]
    tp_peers = [lax.rem(t + d, TP) for d in (4, 5, 3, 2, 6, 7, 1)]

    barrier = pltpu.get_barrier_semaphore()
    for peer in kv_peers:
        pl.semaphore_signal(barrier, inc=1, device_id=(peer, t), device_id_type=MESH)
    for peer in tp_peers:
        pl.semaphore_signal(barrier, inc=1, device_id=(k, peer), device_id_type=MESH)

    def to_kv(phase, src, dst, peer):
        pltpu.make_async_remote_copy(
            src_ref=src,
            dst_ref=dst.at[k],
            send_sem=send_sem.at[phase],
            recv_sem=recv_sem.at[phase],
            device_id=(peer, t),
            device_id_type=MESH,
        ).start()

    def to_tp(phase, src, dst):
        for peer in tp_peers:
            pltpu.make_async_remote_copy(
                src_ref=src,
                dst_ref=dst.at[t],
                send_sem=send_sem.at[phase],
                recv_sem=recv_sem.at[phase],
                device_id=(k, peer),
                device_id_type=MESH,
            ).start()

    def arrived(sems, phase, buffer):
        some = buffer.at[pl.ds(0, buffer.shape[0] - 1)]
        pltpu.make_async_copy(some, some, sems.at[phase]).wait()

    for name in ("tok", "mix"):
        loads[name].wait()
    for s in range(SEQS):
        xs[NEW * s : NEW * s + NEW, :] = tok[s].astype(F32)
    x = xs[...]
    scaled = (x * mix[...]).astype(BF16)
    est[...] = jnp.broadcast_to(jnp.sum(x * x, axis=1, keepdims=True), (ROWS, 128))
    loads["wf"].wait()
    est[:, 0:16] = jnp.dot(scaled, wf[...], preferred_element_type=F32)
    for n, (name, w) in enumerate((("wq", wq), ("wk", wk), ("wv", wv))):
        loads[name].wait()
        part = jnp.dot(scaled, w[...], preferred_element_type=F32)
        for s in range(SEQS):
            for h in range(HEADS):
                send_a[2 * s + h, :, HD * n : HD * n + HD] = part[
                    NEW * s : NEW * s + NEW, HD * h : HD * h + HD
                ].astype(BF16)
    for s in range(SEQS):
        piece = est[NEW * s : NEW * s + NEW, :].astype(BF16)
        for h in range(HEADS):
            send_a[2 * s + h, :, 3 * HD : 4 * HD] = piece
    pl.semaphore_wait(barrier, KV - 1 + TP - 1)
    for peer in kv_peers:
        to_kv(0, send_a.at[peer], recv_a, peer)
    recv_a[pl.ds(k, 1)] = send_a[pl.ds(k, 1)]
    qblk[...] = jnp.zeros(qblk.shape, F32)
    arrived(recv_sem, 0, recv_a)
    total = recv_a[0].astype(F32)
    for j in range(1, KV):
        total = total + recv_a[j].astype(F32)
    inv_norm = lax.rsqrt(total[:, 4 * HD - 1 : 4 * HD] / D + EPSILON)
    query = (inv_norm * total[:, 0:HD]).astype(BF16)
    key_new = (inv_norm * total[:, HD : 2 * HD]).astype(BF16).astype(F32)
    value_new = (inv_norm * total[:, 2 * HD : 3 * HD]).astype(BF16).astype(F32)
    lane = lax.broadcasted_iota(jnp.int32, (NEW, 128), 1)
    forget_sum = jnp.sum(
        jnp.where(lane == 2 * t + head, total[:, 3 * HD :], 0.0), axis=1, keepdims=True
    )
    send_q[0] = query
    for peer in kv_peers:
        to_kv(1, send_q.at[0], recv_q, peer)
    recv_q[pl.ds(k, 1)] = query[None]
    gate_in = inv_norm * forget_sum + bias_ref[head]
    log_forget = jnp.minimum(gate_in, 0.0) - jnp.log1p(jnp.exp(-jnp.abs(gate_in)))

    for name in ("kc", "vc", "cg"):
        loads[name].wait()
    arrived(recv_sem, 1, recv_q)
    for s in range(SEQS):
        for h in range(HEADS):
            qblk[s, NEW * h : NEW * h + NEW, HD * h : HD * h + HD] = recv_q[2 * s + h].astype(F32)
    score_scale = HD**-0.5
    position = k * POS + lax.broadcasted_iota(jnp.int32, (8, POS), 1)
    row8 = lax.broadcasted_iota(jnp.int32, (8, POS), 0)
    lane8 = lax.broadcasted_iota(jnp.int32, (8, 128), 1)

    def one_sequence(s):
        length = lengths_ref[s]
        scores = lax.dot_general(
            qblk[s].astype(BF16), kc[s], (((1,), (1,)), ((), ())), preferred_element_type=F32
        )
        both = cg[s]
        cum = jnp.where(row8 < NEW, both[0:1, :], both[1:2, :])
        live = position < length
        scores = jnp.where(live, scores * score_scale - cum, NEG_FILL)
        peak = jnp.max(scores, axis=1, keepdims=True)
        weights = jnp.where(live, jnp.exp(scores - peak), 0.0)
        block_total = jnp.sum(weights, axis=1, keepdims=True)
        block_sum = jnp.dot(weights.astype(BF16), vc[s], preferred_element_type=F32)
        last = jnp.sum(jnp.where(position == length - 1, cum, 0.0), axis=1, keepdims=True)
        stats = jnp.where(
            lane8 == 0, peak, jnp.where(lane8 == 1, block_total, jnp.where(lane8 == 2, last, 0.0))
        )
        for h in range(HEADS):
            lines = slice(NEW * h, NEW * h + NEW)
            send_b[2 * s + h, :, 0:HD] = block_sum[lines, HD * h : HD * h + HD]
            send_b[2 * s + h, :, HD:] = stats[lines]

    def four_sequences(j, carry):
        order = [lax.rem(mine + 8 + 4 * j + u, SEQS) for u in range(4)]
        for s in order:
            one_sequence(s)
        for s in order:
            for h in range(HEADS):
                peer = 2 * s + h

                @pl.when(peer != k)
                def _():
                    to_kv(2, send_b.at[peer], recv_b, peer)

        return carry

    lax.fori_loop(0, 4, four_sequences, 0)
    recv_b[pl.ds(k, 1)] = send_b[pl.ds(k, 1)]
    arrived(recv_sem, 2, recv_b)

    past_peak = recv_b[0, :, HD : HD + 1]
    for j in range(1, KV):
        past_peak = jnp.maximum(past_peak, recv_b[j, :, HD : HD + 1])
    past_total = jnp.zeros((NEW, 1), F32)
    last_cum = jnp.zeros((NEW, 1), F32)
    past_sum = jnp.zeros((NEW, HD), F32)
    for j in range(KV):
        stats = recv_b[j, :, HD:]
        factor = jnp.exp(stats[:, 0:1] - past_peak)
        past_total = past_total + stats[:, 1:2] * factor
        last_cum = last_cum + stats[:, 2:3]
        past_sum = past_sum + recv_b[j, :, 0:HD] * factor
    query_wide = query.astype(F32)
    token = lax.broadcasted_iota(jnp.int32, (NEW, 1), 0)
    key_cum = last_cum[0:1, :]
    own_scores = []
    for i in range(NEW):
        key_cum = key_cum + log_forget[i : i + 1, :]
        dots = jnp.sum(query_wide * key_new[i : i + 1, :], axis=1, keepdims=True)
        own_scores.append(jnp.where(token >= i, dots * score_scale - key_cum, NEG_FILL))
    peak_score = past_peak
    for score in own_scores:
        peak_score = jnp.maximum(peak_score, score)
    past_factor = jnp.exp(past_peak - peak_score)
    numerator = past_sum * past_factor
    denominator = past_total * past_factor
    for i, score in enumerate(own_scores):
        weight = jnp.where(token >= i, jnp.exp(score - peak_score), 0.0)
        numerator = numerator + weight.astype(BF16).astype(F32) * value_new[i : i + 1, :]
        denominator = denominator + weight
    attended = (numerator / denominator).astype(BF16)
    send_t[0] = attended
    for peer in kv_peers:
        to_kv(3, send_t.at[0], recv_t, peer)
    recv_t[pl.ds(k, 1)] = attended[None]
    loads["wo"].wait()
    arrived(recv_sem, 3, recv_t)
    for s in range(SEQS):
        for h in range(HEADS):
            att[NEW * s : NEW * s + NEW, HD * h : HD * h + HD] = recv_t[2 * s + h].astype(F32)

    send_c[0] = jnp.dot(att[...].astype(BF16), wo[...], preferred_element_type=F32).astype(BF16)
    to_tp(4, send_c.at[0], recv_c)
    recv_c[pl.ds(t, 1)] = send_c[...]
    for name in ("mlp", "wg", "wu"):
        loads[name].wait()
    arrived(recv_sem, 4, recv_c)
    attn_out = recv_c[0].astype(F32)
    for j in range(1, TP):
        attn_out = attn_out + recv_c[j].astype(F32)
    middle = (xs[...] + attn_out).astype(BF16).astype(F32)
    xs[...] = middle
    scaled2 = (middle * mlp[...]).astype(BF16)
    squares = jnp.broadcast_to(jnp.sum(middle * middle, axis=1, keepdims=True), (ROWS, 128))
    rough = squares.astype(BF16).astype(F32)
    lane64 = lax.broadcasted_iota(jnp.int32, (ROWS, 128), 1)
    est[...] = jnp.where(lane64 < 64, rough, squares - rough)

    for half in range(2):
        for s in range(SEQS):
            send_e[2 * s + half, :, 2 * HALF :] = est[NEW * s : NEW * s + NEW, :].astype(BF16)
        for n, w in enumerate((wg, wu)):
            for c in range(0, HALF, 256):
                begin = SHIFT * half + c
                part = jnp.dot(scaled2, w[:, begin : begin + 256], preferred_element_type=F32)
                for s in range(SEQS):
                    send_e[2 * s + half, :, HALF * n + c : HALF * n + c + 256] = part[
                        NEW * s : NEW * s + NEW
                    ].astype(BF16)
        for j in range(SEQS):
            peer = 2 * lax.rem(mine + 8 + j, SEQS) + half

            @pl.when(peer != k)
            def _():
                to_kv(5, send_e.at[peer], recv_e, peer)

    recv_e[pl.ds(k, 1)] = send_e[pl.ds(k, 1)]
    arrived(recv_sem, 5, recv_e)
    total = recv_e[0].astype(F32)
    for j in range(1, KV):
        total = total + recv_e[j].astype(F32)
    square_sum = total[:, 2 * HALF : 2 * HALF + 1] + total[:, 2 * HALF + 127 : 2 * HALF + 128]
    inv_norm2 = lax.rsqrt(square_sum / D + EPSILON)
    gate = inv_norm2 * total[:, 0:HALF]
    up = inv_norm2 * total[:, HALF : 2 * HALF]
    hidden = (gate * jax.nn.sigmoid(gate) * up).astype(BF16)
    send_h[0] = hidden
    for peer in kv_peers:
        to_kv(6, send_h.at[0], recv_h, peer)
    recv_h[pl.ds(k, 1)] = hidden[None]
    loads["wd"].wait()
    arrived(recv_sem, 6, recv_h)
    for s in range(SEQS):
        hid[NEW * s : NEW * s + NEW, 0:HALF] = recv_h[2 * s].astype(F32)
        hid[NEW * s : NEW * s + NEW, HALF:] = recv_h[2 * s + 1, :, HALF - SHIFT :].astype(F32)

    send_f[0] = jnp.dot(hid[...].astype(BF16), wd[...], preferred_element_type=F32).astype(BF16)
    to_tp(7, send_f.at[0], recv_f)
    recv_f[pl.ds(t, 1)] = send_f[...]
    arrived(recv_sem, 7, recv_f)
    mixed = recv_f[0].astype(F32)
    for j in range(1, TP):
        mixed = mixed + recv_f[j].astype(F32)
    out_ref[...] = (xs[...] + mixed).astype(BF16)

    for phase, buffer in enumerate(
        (recv_a, recv_q, recv_b, recv_t, recv_c, recv_e, recv_h, recv_f)
    ):
        arrived(send_sem, phase, buffer)


def on_device(
    tokens,
    mix_gain,
    w_query,
    w_key,
    w_value,
    w_forget,
    forget_bias,
    key_cache,
    value_cache,
    cum_gate,
    lengths,
    w_out,
    mlp_gain,
    w_gate,
    w_up,
    w_down,
):
    in_vmem = [
        tokens,
        mix_gain.reshape(1, WIDTH),
        w_query,
        w_key,
        w_value,
        w_forget,
        key_cache,
        value_cache,
        cum_gate,
        w_out,
        mlp_gain.reshape(1, WIDTH),
        w_gate,
        w_up,
        w_down,
    ]
    shapes = [pltpu.VMEM(a.shape, a.dtype) for a in in_vmem]
    shapes[5] = pltpu.VMEM((WIDTH, 16), BF16)
    out = pl.pallas_call(
        kernel,
        out_shape=jax.ShapeDtypeStruct((ROWS, WIDTH), BF16),
        in_specs=[pl.BlockSpec(memory_space=pltpu.SMEM)] * 2
        + [pl.BlockSpec(memory_space=pl.ANY)] * len(in_vmem),
        out_specs=pl.BlockSpec(memory_space=pltpu.VMEM),
        scratch_shapes=shapes
        + [
            pltpu.VMEM((ROWS, WIDTH), F32),
            pltpu.VMEM((ROWS, 128), F32),
            pltpu.VMEM((SEQS, 8, 2 * HD), F32),
            pltpu.VMEM((ROWS, 2 * HD), F32),
            pltpu.VMEM((ROWS, FF), F32),
            pltpu.VMEM((KV, NEW, 4 * HD), BF16),
            pltpu.VMEM((KV, NEW, 4 * HD), BF16),
            pltpu.VMEM((1, NEW, HD), BF16),
            pltpu.VMEM((KV, NEW, HD), BF16),
            pltpu.VMEM((KV, NEW, 2 * HD), F32),
            pltpu.VMEM((KV, NEW, 2 * HD), F32),
            pltpu.VMEM((1, NEW, HD), BF16),
            pltpu.VMEM((KV, NEW, HD), BF16),
            pltpu.VMEM((1, ROWS, WIDTH), BF16),
            pltpu.VMEM((TP, ROWS, WIDTH), BF16),
            pltpu.VMEM((KV, NEW, 2 * HALF + 128), BF16),
            pltpu.VMEM((KV, NEW, 2 * HALF + 128), BF16),
            pltpu.VMEM((1, NEW, HALF), BF16),
            pltpu.VMEM((KV, NEW, HALF), BF16),
            pltpu.VMEM((1, ROWS, WIDTH), BF16),
            pltpu.VMEM((TP, ROWS, WIDTH), BF16),
            pltpu.SemaphoreType.DMA((len(in_vmem),)),
            pltpu.SemaphoreType.DMA((8,)),
            pltpu.SemaphoreType.DMA((8,)),
        ],
        compiler_params=pltpu.CompilerParams(
            collective_id=0, has_side_effects=True, vmem_limit_bytes=48 * 1024 * 1024
        ),
    )(lengths, forget_bias, *in_vmem)
    return out.reshape(SEQS, NEW, WIDTH)


def solution(mesh):
    return jax.shard_map(
        on_device,
        mesh=mesh,
        in_specs=(
            P(None, None, "kv"),
            P("kv"),
            P("kv", "tp"),
            P("kv", "tp"),
            P("kv", "tp"),
            P(),
            P("tp"),
            P(None, "kv", "tp"),
            P(None, "kv", "tp"),
            P(None, "tp", "kv"),
            P(),
            P("tp", "kv"),
            P("kv"),
            P("kv", "tp"),
            P("kv", "tp"),
            P("tp", "kv"),
        ),
        out_specs=P(None, None, "kv"),
        check_vma=False,
    )
```

```python
import jax
import jax.numpy as jnp
from jax import lax
from jax.experimental import pallas as pl
from jax.experimental.pallas import tpu as pltpu
from jax.sharding import PartitionSpec as P

D = 4096
EPSILON = 1e-06
NEG_FILL = -1e30
PEAK_FLOOR = -1e29
SEQS = 16
NEW = 4
ROWS = SEQS * NEW
HEADS = 2
HD = 128
WIDTH = 128
POS = 512
FF = 1408
CUT = 768
FIRST = 384
EARLY = 128 + 2 * FIRST
LATE = (2 * (CUT - FIRST), 2 * (FF - CUT - FIRST))
KV = 32
TP = 8
ZS, YS = 8, 4
F32 = jnp.float32
BF16 = jnp.bfloat16
MESH = pl.DeviceIdType.MESH


OFFSETS = sorted(
    ((dz, dy) for dz in range(ZS) for dy in range(YS) if dz or dy),
    key=lambda o: -(min(o[0], ZS - o[0]) + min(o[1], YS - o[1])),
)


def kernel(
    lengths_ref,
    bias_ref,
    tokens_hbm,
    mix_hbm,
    wq_hbm,
    wk_hbm,
    wv_hbm,
    wf_hbm,
    kc_hbm,
    vc_hbm,
    cg_hbm,
    wo_hbm,
    mlp_hbm,
    wg_hbm,
    wu_hbm,
    wd_hbm,
    out_ref,
    tok,
    mix,
    wq,
    wk,
    wv,
    wf,
    kc,
    vc,
    cg,
    wo,
    mlp,
    wg,
    wu,
    wd,
    xs,
    est,
    qblk,
    bias,
    last,
    att,
    hid,
    send_a,
    recv_a,
    send_q,
    recv_q,
    send_b,
    recv_b,
    send_t,
    recv_t,
    send_c,
    recv_c,
    send_e,
    recv_e,
    send_l,
    recv_l,
    send_h,
    recv_h,
    send_m,
    recv_m,
    send_f,
    recv_f,
    in_sem,
    send_sem,
    recv_sem,
):
    k = lax.axis_index("kv")
    t = lax.axis_index("tp")
    z, y = k // YS, lax.rem(k, YS)
    head = lax.rem(k, 2)
    mine = k // 2

    loads = {}
    sources = dict(
        tok=(tokens_hbm, tok),
        mix=(mix_hbm, mix),
        wq=(wq_hbm, wq),
        wk=(wk_hbm, wk),
        wv=(wv_hbm, wv),
        wf=(wf_hbm.at[:, pl.ds(pl.multiple_of(k * WIDTH, WIDTH), WIDTH)], wf),
        kc=(kc_hbm, kc),
        vc=(vc_hbm, vc),
        cg=(cg_hbm, cg),
        wo=(wo_hbm, wo),
        mlp=(mlp_hbm, mlp),
        wg=(wg_hbm, wg),
        wu=(wu_hbm, wu),
        wd=(wd_hbm, wd),
    )
    for n, (name, (src, dst)) in enumerate(sources.items()):
        loads[name] = pltpu.make_async_copy(src, dst, in_sem.at[n])
        loads[name].start()

    kv_peers = [lax.rem(z + dz, ZS) * YS + lax.rem(y + dy, YS) for dz, dy in OFFSETS]
    tp_peers = [lax.rem(t + d, TP) for d in (4, 5, 3, 2, 6, 7, 1)]

    barrier = pltpu.get_barrier_semaphore()
    for peer in kv_peers:
        pl.semaphore_signal(barrier, inc=1, device_id=(peer, t), device_id_type=MESH)
    for peer in tp_peers:
        pl.semaphore_signal(barrier, inc=1, device_id=(k, peer), device_id_type=MESH)

    def to_kv(phase, src, dst, peer):
        pltpu.make_async_remote_copy(
            src_ref=src,
            dst_ref=dst.at[k],
            send_sem=send_sem.at[phase],
            recv_sem=recv_sem.at[phase],
            device_id=(peer, t),
            device_id_type=MESH,
        ).start()

    def to_kv_part(phase, src, dst, peer, width, at=None):
        pltpu.make_async_remote_copy(
            src_ref=src.at[peer if at is None else at, :, pl.ds(0, width)],
            dst_ref=dst.at[k, :, pl.ds(0, width)],
            send_sem=send_sem.at[phase],
            recv_sem=recv_sem.at[phase],
            device_id=(peer, t),
            device_id_type=MESH,
        ).start()

    def to_tp(phase, src, dst):
        for peer in tp_peers:
            pltpu.make_async_remote_copy(
                src_ref=src,
                dst_ref=dst.at[t],
                send_sem=send_sem.at[phase],
                recv_sem=recv_sem.at[phase],
                device_id=(k, peer),
                device_id_type=MESH,
            ).start()

    def arrived(sems, phase, buffer):
        some = buffer.at[pl.ds(0, buffer.shape[0] - 1)]
        with jax.named_scope(("recv%d" if sems is recv_sem else "sent%d") % phase):
            pltpu.make_async_copy(some, some, sems.at[phase]).wait()

    for name in ("tok", "mix"):
        loads[name].wait()
    for s in range(SEQS):
        xs[NEW * s : NEW * s + NEW, :] = tok[s].astype(F32)
    x = xs[...]
    scaled = (x * mix[...]).astype(BF16)
    est[...] = jnp.broadcast_to(jnp.sum(x * x, axis=1, keepdims=True), (ROWS, 128))
    loads["wf"].wait()
    est[:, 0:16] = lax.dot_general(
        scaled, wf[...], (((1,), (1,)), ((), ())), preferred_element_type=F32
    )
    for n, (name, w) in enumerate((("wq", wq), ("wk", wk), ("wv", wv))):
        loads[name].wait()
        part = jnp.dot(scaled, w[...], preferred_element_type=F32)
        for s in range(SEQS):
            for h in range(HEADS):
                send_a[2 * s + h, :, HD * n : HD * n + HD] = part[
                    NEW * s : NEW * s + NEW, HD * h : HD * h + HD
                ].astype(BF16)
    for s in range(SEQS):
        piece = est[NEW * s : NEW * s + NEW, :].astype(BF16)
        for h in range(HEADS):
            send_a[2 * s + h, :, 3 * HD : 4 * HD] = piece
    with jax.named_scope("barrier"):
        pl.semaphore_wait(barrier, KV - 1 + TP - 1)
    for peer in kv_peers:
        to_kv(0, send_a.at[peer], recv_a, peer)
    recv_a[pl.ds(k, 1)] = send_a[pl.ds(k, 1)]
    qblk[...] = jnp.zeros(qblk.shape, F32)
    for name in ("kc", "vc", "cg"):
        loads[name].wait()
    score_scale = HD**-0.5
    position = k * POS + lax.broadcasted_iota(jnp.int32, (8, POS), 1)
    row8 = lax.broadcasted_iota(jnp.int32, (8, POS), 0)
    lane8 = lax.broadcasted_iota(jnp.int32, (8, 128), 1)
    for s in range(SEQS):
        length = lengths_ref[s]
        both = cg[s]
        cum = jnp.where(row8 < NEW, both[0:1, :], both[1:2, :])
        bias[s] = jnp.where(position < length, -cum, NEG_FILL)
        at_last = jnp.sum(jnp.where(position == length - 1, cum, 0.0), axis=1, keepdims=True)
        last[s] = jnp.broadcast_to(at_last, (8, 128))
    arrived(recv_sem, 0, recv_a)
    total = recv_a[0].astype(F32)
    for j in range(1, KV):
        total = total + recv_a[j].astype(F32)
    inv_norm = lax.rsqrt(total[:, 4 * HD - 1 : 4 * HD] / D + EPSILON)
    query = (inv_norm * total[:, 0:HD]).astype(BF16)
    key_new = (inv_norm * total[:, HD : 2 * HD]).astype(BF16).astype(F32)
    value_new = (inv_norm * total[:, 2 * HD : 3 * HD]).astype(BF16).astype(F32)
    lane = lax.broadcasted_iota(jnp.int32, (NEW, 128), 1)
    forget_sum = jnp.sum(
        jnp.where(lane == 2 * t + head, total[:, 3 * HD :], 0.0), axis=1, keepdims=True
    )
    send_q[0] = query
    for peer in kv_peers:
        to_kv(1, send_q.at[0], recv_q, peer)
    recv_q[pl.ds(k, 1)] = query[None]
    gate_in = inv_norm * forget_sum + bias_ref[head]
    log_forget = jnp.minimum(gate_in, 0.0) - jnp.log1p(jnp.exp(-jnp.abs(gate_in)))

    arrived(recv_sem, 1, recv_q)
    for s in range(SEQS):
        for h in range(HEADS):
            qblk[s, NEW * h : NEW * h + NEW, HD * h : HD * h + HD] = recv_q[2 * s + h].astype(F32)
    for dz in (4, 5, 3, 6, 2, 7, 1, 0):
        z_peer = lax.rem(z + dz, ZS)
        for s in (2 * z_peer, 2 * z_peer + 1):
            scores = lax.dot_general(
                qblk[s].astype(BF16), kc[s], (((1,), (1,)), ((), ())), preferred_element_type=F32
            )
            scores = scores * score_scale + bias[s]
            peak = jnp.maximum(jnp.max(scores, axis=1, keepdims=True), PEAK_FLOOR)
            weights = jnp.exp(scores - peak)
            block_total = jnp.sum(weights, axis=1, keepdims=True)
            block_sum = jnp.dot(weights.astype(BF16), vc[s], preferred_element_type=F32)
            stats = jnp.where(lane8 == 0, peak, jnp.where(lane8 == 1, block_total, last[s]))
            for h in range(HEADS):
                lines = slice(NEW * h, NEW * h + NEW)
                send_b[2 * s + h, :, 0:HD] = block_sum[lines, HD * h : HD * h + HD]
                send_b[2 * s + h, :, HD:] = stats[lines]
        for dy in (2, 1, 3, 0):
            if dz or dy:
                peer = z_peer * YS + lax.rem(y + dy, YS)
                to_kv(2, send_b.at[peer], recv_b, peer)
    recv_b[pl.ds(k, 1)] = send_b[pl.ds(k, 1)]
    arrived(recv_sem, 2, recv_b)

    past_peak = recv_b[0, :, HD : HD + 1]
    for j in range(1, KV):
        past_peak = jnp.maximum(past_peak, recv_b[j, :, HD : HD + 1])
    past_total = jnp.zeros((NEW, 1), F32)
    last_cum = jnp.zeros((NEW, 1), F32)
    past_sum = jnp.zeros((NEW, HD), F32)
    for j in range(KV):
        stats = recv_b[j, :, HD:]
        factor = jnp.exp(stats[:, 0:1] - past_peak)
        past_total = past_total + stats[:, 1:2] * factor
        last_cum = last_cum + stats[:, 2:3]
        past_sum = past_sum + recv_b[j, :, 0:HD] * factor
    query_wide = query.astype(F32)
    token = lax.broadcasted_iota(jnp.int32, (NEW, 1), 0)
    key_cum = last_cum[0:1, :]
    own_scores = []
    for i in range(NEW):
        key_cum = key_cum + log_forget[i : i + 1, :]
        dots = jnp.sum(query_wide * key_new[i : i + 1, :], axis=1, keepdims=True)
        own_scores.append(jnp.where(token >= i, dots * score_scale - key_cum, NEG_FILL))
    peak_score = past_peak
    for score in own_scores:
        peak_score = jnp.maximum(peak_score, score)
    past_factor = jnp.exp(past_peak - peak_score)
    numerator = past_sum * past_factor
    denominator = past_total * past_factor
    for i, score in enumerate(own_scores):
        weight = jnp.where(token >= i, jnp.exp(score - peak_score), 0.0)
        numerator = numerator + weight.astype(BF16).astype(F32) * value_new[i : i + 1, :]
        denominator = denominator + weight
    attended = (numerator / denominator).astype(BF16)
    send_t[0] = attended
    for peer in kv_peers:
        to_kv(3, send_t.at[0], recv_t, peer)
    recv_t[pl.ds(k, 1)] = attended[None]
    loads["wo"].wait()
    arrived(recv_sem, 3, recv_t)
    for s in range(SEQS):
        for h in range(HEADS):
            att[NEW * s : NEW * s + NEW, HD * h : HD * h + HD] = recv_t[2 * s + h].astype(F32)

    send_c[0] = jnp.dot(att[...].astype(BF16), wo[...], preferred_element_type=F32).astype(BF16)
    to_tp(4, send_c.at[0], recv_c)
    recv_c[pl.ds(t, 1)] = send_c[...]
    for name in ("mlp", "wg", "wu"):
        loads[name].wait()
    arrived(recv_sem, 4, recv_c)
    attn_out = recv_c[0].astype(F32)
    for j in range(1, TP):
        attn_out = attn_out + recv_c[j].astype(F32)
    middle = (xs[...] + attn_out).astype(BF16).astype(F32)
    xs[...] = middle
    scaled2 = (middle * mlp[...]).astype(BF16)
    squares = jnp.broadcast_to(jnp.sum(middle * middle, axis=1, keepdims=True), (ROWS, 128))
    rough = squares.astype(BF16).astype(F32)
    lane64 = lax.broadcasted_iota(jnp.int32, (ROWS, 128), 1)
    est[...] = jnp.where(lane64 < 64, rough, squares - rough)

    for s in range(SEQS):
        piece = est[NEW * s : NEW * s + NEW, :].astype(BF16)
        for half in range(2):
            send_e[2 * s + half, :, 0:128] = piece

    def partial_products(dst, at, begin, width, half):
        for n, w in enumerate((wg, wu)):
            part = jnp.dot(scaled2, w[:, begin : begin + width], preferred_element_type=F32)
            for s in range(SEQS):
                dst[2 * s + half, :, at + width * n : at + width * n + width] = part[
                    NEW * s : NEW * s + NEW
                ].astype(BF16)

    for half in range(2):
        partial_products(send_e, 128, CUT * half, FIRST, half)
    for peer in kv_peers:
        to_kv(5, send_e.at[peer], recv_e, peer)
    for half in range(2):
        partial_products(send_l, 0, CUT * half + FIRST, LATE[half] // 2, half)
    for dz, dy in OFFSETS:
        peer = lax.rem(z + dz, ZS) * YS + lax.rem(y + dy, YS)
        half = lax.rem(y + dy, 2)
        for h in range(2):

            @pl.when(half == h)
            def _():
                to_kv_part(8, send_l, recv_l, peer, LATE[h])

    recv_e[pl.ds(k, 1)] = send_e[pl.ds(k, 1)]
    recv_l[pl.ds(k, 1)] = send_l[pl.ds(k, 1)]
    arrived(recv_sem, 5, recv_e)
    total = recv_e[0].astype(F32)
    for j in range(1, KV):
        total = total + recv_e[j].astype(F32)
    inv_norm2 = lax.rsqrt((total[:, 0:1] + total[:, 127:128]) / D + EPSILON)

    def hidden_of(gate, up):
        gate = inv_norm2 * gate
        return (gate * jax.nn.sigmoid(gate) * (inv_norm2 * up)).astype(BF16)

    hidden = hidden_of(total[:, 128 : 128 + FIRST], total[:, 128 + FIRST :])
    send_h[0] = hidden
    for peer in kv_peers:
        to_kv(6, send_h.at[0], recv_h, peer)
    recv_h[pl.ds(k, 1)] = hidden[None]
    for h in range(2):

        @pl.when(head == h)
        def _():
            width = LATE[h]
            with jax.named_scope("recv8"):
                some = recv_l.at[pl.ds(0, KV - 1), :, pl.ds(0, width)]
                pltpu.make_async_copy(some, some, recv_sem.at[8]).wait()
            total = recv_l[0, :, 0:width].astype(F32)
            for j in range(1, KV):
                total = total + recv_l[j, :, 0:width].astype(F32)
            hidden = hidden_of(total[:, 0 : width // 2], total[:, width // 2 :])
            send_m[0, :, 0 : width // 2] = hidden
            recv_m[pl.ds(k, 1), :, 0 : width // 2] = hidden[None]
            for peer in kv_peers:
                to_kv_part(9, send_m, recv_m, peer, width // 2, 0)

    loads["wd"].wait()
    arrived(recv_sem, 6, recv_h)
    for s in range(SEQS):
        for h in range(2):
            hid[NEW * s : NEW * s + NEW, CUT * h : CUT * h + FIRST] = recv_h[2 * s + h].astype(F32)
    enough = (recv_e.at[pl.ds(0, 11)], recv_l.at[pl.ds(0, 13)])
    for h in range(2):

        @pl.when(head == h)
        def _():
            with jax.named_scope("recv9"):
                pltpu.make_async_copy(enough[h], enough[h], recv_sem.at[9]).wait()

    for s in range(SEQS):
        for h in range(2):
            begin, width = CUT * h + FIRST, LATE[h] // 2
            hid[NEW * s : NEW * s + NEW, begin : begin + width] = recv_m[
                2 * s + h, :, 0:width
            ].astype(F32)

    send_f[0] = jnp.dot(hid[...].astype(BF16), wd[...], preferred_element_type=F32).astype(BF16)
    to_tp(7, send_f.at[0], recv_f)
    recv_f[pl.ds(t, 1)] = send_f[...]
    arrived(recv_sem, 7, recv_f)
    mixed = recv_f[0].astype(F32)
    for j in range(1, TP):
        mixed = mixed + recv_f[j].astype(F32)
    out_ref[...] = (xs[...] + mixed).astype(BF16)

    for phase, buffer in enumerate(
        (recv_a, recv_q, recv_b, recv_t, recv_c, recv_e, recv_h, recv_f)
    ):
        arrived(send_sem, phase, buffer)
    enough = (recv_e.at[pl.ds(0, 22)], recv_l.at[pl.ds(0, 26)])
    for h in range(2):

        @pl.when(head == h)
        def _():
            pltpu.make_async_copy(enough[h], enough[h], send_sem.at[8]).wait()
            some = recv_m.at[pl.ds(0, KV - 1), :, pl.ds(0, LATE[h] // 2)]
            pltpu.make_async_copy(some, some, send_sem.at[9]).wait()


def on_device(
    tokens,
    mix_gain,
    w_query,
    w_key,
    w_value,
    w_forget,
    forget_bias,
    key_cache,
    value_cache,
    cum_gate,
    lengths,
    w_out,
    mlp_gain,
    w_gate,
    w_up,
    w_down,
):
    in_vmem = [
        tokens,
        mix_gain.reshape(1, WIDTH),
        w_query,
        w_key,
        w_value,
        w_forget.T,
        key_cache,
        value_cache,
        cum_gate,
        w_out,
        mlp_gain.reshape(1, WIDTH),
        w_gate,
        w_up,
        w_down,
    ]
    shapes = [pltpu.VMEM(a.shape, a.dtype) for a in in_vmem]
    shapes[5] = pltpu.VMEM((16, WIDTH), BF16)
    out = pl.pallas_call(
        kernel,
        out_shape=jax.ShapeDtypeStruct((ROWS, WIDTH), BF16),
        in_specs=[pl.BlockSpec(memory_space=pltpu.SMEM)] * 2
        + [pl.BlockSpec(memory_space=pltpu.HBM)] * len(in_vmem),
        out_specs=pl.BlockSpec(memory_space=pltpu.VMEM),
        scratch_shapes=shapes
        + [
            pltpu.VMEM((ROWS, WIDTH), F32),
            pltpu.VMEM((ROWS, 128), F32),
            pltpu.VMEM((SEQS, 8, 2 * HD), F32),
            pltpu.VMEM((SEQS, 8, POS), F32),
            pltpu.VMEM((SEQS, 8, 128), F32),
            pltpu.VMEM((ROWS, 2 * HD), F32),
            pltpu.VMEM((ROWS, FF), F32),
            pltpu.VMEM((KV, NEW, 4 * HD), BF16),
            pltpu.VMEM((KV, NEW, 4 * HD), BF16),
            pltpu.VMEM((1, NEW, HD), BF16),
            pltpu.VMEM((KV, NEW, HD), BF16),
            pltpu.VMEM((KV, NEW, 2 * HD), F32),
            pltpu.VMEM((KV, NEW, 2 * HD), F32),
            pltpu.VMEM((1, NEW, HD), BF16),
            pltpu.VMEM((KV, NEW, HD), BF16),
            pltpu.VMEM((1, ROWS, WIDTH), BF16),
            pltpu.VMEM((TP, ROWS, WIDTH), BF16),
            pltpu.VMEM((KV, NEW, EARLY), BF16),
            pltpu.VMEM((KV, NEW, EARLY), BF16),
            pltpu.VMEM((KV, NEW, LATE[0]), BF16),
            pltpu.VMEM((KV, NEW, LATE[0]), BF16),
            pltpu.VMEM((1, NEW, FIRST), BF16),
            pltpu.VMEM((KV, NEW, FIRST), BF16),
            pltpu.VMEM((1, NEW, LATE[0] // 2), BF16),
            pltpu.VMEM((KV, NEW, LATE[0] // 2), BF16),
            pltpu.VMEM((1, ROWS, WIDTH), BF16),
            pltpu.VMEM((TP, ROWS, WIDTH), BF16),
            pltpu.SemaphoreType.DMA((len(in_vmem),)),
            pltpu.SemaphoreType.DMA((10,)),
            pltpu.SemaphoreType.DMA((10,)),
        ],
        compiler_params=pltpu.CompilerParams(
            collective_id=0, has_side_effects=True, vmem_limit_bytes=67043328
        ),
    )(lengths, forget_bias, *in_vmem)
    return out.reshape(SEQS, NEW, WIDTH)


def solution(mesh):
    return jax.shard_map(
        on_device,
        mesh=mesh,
        in_specs=(
            P(None, None, "kv"),
            P("kv"),
            P("kv", "tp"),
            P("kv", "tp"),
            P("kv", "tp"),
            P(),
            P("tp"),
            P(None, "kv", "tp"),
            P(None, "kv", "tp"),
            P(None, "tp", "kv"),
            P(),
            P("tp", "kv"),
            P("kv"),
            P("kv", "tp"),
            P("kv", "tp"),
            P("tp", "kv"),
        ),
        out_specs=P(None, None, "kv"),
        check_vma=False,
    )
```

```python
import jax
import jax.numpy as jnp
from jax import lax
from jax.experimental import pallas as pl
from jax.experimental.pallas import tpu as pltpu
from jax.sharding import PartitionSpec as P

D = 4096
EPSILON = 1e-06
NEG_FILL = -1e30
PEAK_FLOOR = -1e29
SEQS = 16
NEW = 4
ROWS = SEQS * NEW
HEADS = 2
HD = 128
WIDTH = 128
POS = 512
FF = 1408
CUT = 768
FIRST = 384
EARLY = 128 + 2 * FIRST
LATE = (2 * (CUT - FIRST), 2 * (FF - CUT - FIRST))
KV = 32
TP = 8
ZS, YS = 8, 4
F32 = jnp.float32
BF16 = jnp.bfloat16
MESH = pl.DeviceIdType.MESH


OFFSETS = sorted(
    ((dz, dy) for dz in range(ZS) for dy in range(YS) if dz or dy),
    key=lambda o: -(min(o[0], ZS - o[0]) + min(o[1], YS - o[1])),
)


def kernel(
    lengths_ref,
    bias_ref,
    tokens_hbm,
    mix_hbm,
    wq_hbm,
    wk_hbm,
    wv_hbm,
    wf_hbm,
    kc_hbm,
    vc_hbm,
    cg_hbm,
    wo_hbm,
    mlp_hbm,
    wg_hbm,
    wu_hbm,
    wd_hbm,
    out_ref,
    tok,
    mix,
    wq,
    wk,
    wv,
    wf,
    kc,
    vc,
    cg,
    wo,
    mlp,
    wg,
    wu,
    wd,
    xs,
    est,
    qblk,
    kt,
    bias,
    last,
    att,
    hid,
    state,
    send_a,
    recv_a,
    send_q,
    recv_q,
    send_b,
    recv_b,
    send_t,
    recv_t,
    send_c,
    recv_c,
    send_e,
    recv_e,
    send_l,
    recv_l,
    send_h,
    recv_h,
    send_m,
    recv_m,
    send_f,
    recv_f,
    in_sem,
    send_sem,
    recv_sem,
):
    k = lax.axis_index("kv")
    t = lax.axis_index("tp")
    z, y = k // YS, lax.rem(k, YS)
    head = lax.rem(k, 2)
    mine = k // 2

    loads = {}
    sources = dict(
        tok=(tokens_hbm, tok),
        mix=(mix_hbm, mix),
        wq=(wq_hbm, wq),
        wk=(wk_hbm, wk),
        wv=(wv_hbm, wv),
        wf=(wf_hbm.at[:, pl.ds(pl.multiple_of(k * WIDTH, WIDTH), WIDTH)], wf),
        kc=(kc_hbm, kc),
        vc=(vc_hbm, vc),
        cg=(cg_hbm, cg),
        wo=(wo_hbm, wo),
        mlp=(mlp_hbm, mlp),
        wg=(wg_hbm, wg),
        wu=(wu_hbm, wu),
        wd=(wd_hbm, wd),
    )
    kv_peers = [lax.rem(z + dz, ZS) * YS + lax.rem(y + dy, YS) for dz, dy in OFFSETS]
    tp_peers = [lax.rem(t + d, TP) for d in (4, 5, 3, 2, 6, 7, 1)]
    core = lax.rem(t, 2)
    owner_t = t + 1 - core
    is_owner = core == 1
    no_owner = core == 0

    barrier = pltpu.get_barrier_semaphore()

    def greet(kv, tp):
        pl.semaphore_signal(barrier, inc=1, device_id=(kv, tp), device_id_type=MESH)

    for peer in kv_peers:
        greet(peer, owner_t)

    @pl.when(is_owner)
    def _():
        for peer in kv_peers:
            greet(peer, t - 1)

    for peer in tp_peers:
        greet(k, peer)

    for n, (name, (src, dst)) in enumerate(sources.items()):
        loads[name] = pltpu.make_async_copy(src, dst, in_sem.at[n])
        loads[name].start()

    def send(src, dst, sent, received, kv, tp):
        pltpu.make_async_remote_copy(
            src_ref=src,
            dst_ref=dst,
            send_sem=sent,
            recv_sem=received,
            device_id=(kv, tp),
            device_id_type=MESH,
        ).start()

    def lanes(ref, width):
        return ref if width is None else ref.at[:, pl.ds(0, width)]

    def to_owner(phase, src, dst, peer, width=None):
        send(
            lanes(src.at[peer], width),
            lanes(dst.at[core, k], width),
            send_sem.at[phase, 0],
            recv_sem.at[phase, core],
            peer,
            owner_t,
        )

    def own_to_owner(phase, src, dst, width=None):
        @pl.when(no_owner)
        def _():
            to_owner(phase, src, dst, k, width)

        @pl.when(is_owner)
        def _():
            dst[1, pl.ds(k, 1)] = src[pl.ds(k, 1)]

    def to_members(phase, src, dst, group, width=None):
        peers = kv_peers if group else kv_peers + [k]
        for peer in peers:
            send(
                lanes(src.at[group], width),
                lanes(dst.at[k], width),
                send_sem.at[phase, group],
                recv_sem.at[phase, 0],
                peer,
                t - 1 + group,
            )

    def to_tp(phase, src, dst):
        for peer in tp_peers:
            send(src, dst.at[t], send_sem.at[phase, 0], recv_sem.at[phase, 0], k, peer)

    def wait_bytes(ref, sem):
        pltpu.make_async_copy(ref, ref, sem).wait()

    def arrived_at_owner(phase, dst, group, width=None):
        count = KV - group
        some = dst.at[group, pl.ds(0, count)]
        if width is not None:
            some = dst.at[group, pl.ds(0, count), :, pl.ds(0, width)]
        with jax.named_scope("own%d_%d" % (phase, group)):
            wait_bytes(some, recv_sem.at[phase, group])

    def arrived_at_member(phase, dst):
        for group, role in ((0, no_owner), (1, is_owner)):

            @pl.when(role)
            def _():
                with jax.named_scope("recv%d" % phase):
                    wait_bytes(dst.at[pl.ds(0, KV - group)], recv_sem.at[phase, 0])

    def arrived_tp(phase, dst):
        with jax.named_scope("recv%d" % phase):
            wait_bytes(dst.at[pl.ds(0, TP - 1)], recv_sem.at[phase, 0])

    for name in ("tok", "mix"):
        loads[name].wait()
    for s in range(SEQS):
        xs[NEW * s : NEW * s + NEW, :] = tok[s].astype(F32)
    x = xs[...]
    scaled = (x * mix[...]).astype(BF16)
    est[...] = jnp.broadcast_to(jnp.sum(x * x, axis=1, keepdims=True), (ROWS, 128))
    loads["wf"].wait()
    est[:, 0:16] = lax.dot_general(
        scaled, wf[...], (((1,), (1,)), ((), ())), preferred_element_type=F32
    )
    lane64 = lax.broadcasted_iota(jnp.int32, (ROWS, 128), 1)
    bias_all = jnp.where(lax.rem(lane64, 2) == 0, bias_ref[0], bias_ref[1])
    high = bias_all.astype(BF16).astype(F32)
    middle_part = (bias_all - high).astype(BF16).astype(F32)
    low = bias_all - high - middle_part
    parts = jnp.where(lane64 < 18, high, jnp.where(lane64 < 20, middle_part, low))
    est[...] = jnp.where((lane64 >= 16) & (lane64 < 22), parts, est[...])
    for n, (name, w) in enumerate((("wq", wq), ("wk", wk), ("wv", wv))):
        loads[name].wait()
        part = jnp.dot(scaled, w[...], preferred_element_type=F32)
        for s in range(SEQS):
            for h in range(HEADS):
                send_a[2 * s + h, :, HD * n : HD * n + HD] = part[
                    NEW * s : NEW * s + NEW, HD * h : HD * h + HD
                ].astype(BF16)
    for s in range(SEQS):
        piece = est[NEW * s : NEW * s + NEW, :].astype(BF16)
        for h in range(HEADS):
            send_a[2 * s + h, :, 3 * HD : 4 * HD] = piece
    with jax.named_scope("barrier"):
        pl.semaphore_wait(barrier, KV - 1 + TP - 1 + (KV - 1) * core)
    for peer in kv_peers:
        to_owner(0, send_a, recv_a, peer)
    own_to_owner(0, send_a, recv_a)

    qblk[...] = jnp.zeros(qblk.shape, F32)
    for name in ("kc", "vc", "cg"):
        loads[name].wait()
    score_scale = HD**-0.5
    position = k * POS + lax.broadcasted_iota(jnp.int32, (8, POS), 1)
    row8 = lax.broadcasted_iota(jnp.int32, (8, POS), 0)
    lane8 = lax.broadcasted_iota(jnp.int32, (8, 128), 1)
    for s in range(SEQS):
        length = lengths_ref[s]
        both = cg[s]
        cum = jnp.where(row8 < NEW, both[0:1, :], both[1:2, :])
        bias[s] = jnp.where(position < length, -cum, NEG_FILL)
        at_last = jnp.sum(jnp.where(position == length - 1, cum, 0.0), axis=1, keepdims=True)
        last[s] = jnp.broadcast_to(at_last, (8, 128))
    for s in range(SEQS):
        kt[s] = kc[s].T

    lane = lax.broadcasted_iota(jnp.int32, (NEW, 128), 1)

    @pl.when(is_owner)
    def _():
        for group in (1, 0):
            arrived_at_owner(0, recv_a, group)
            total = recv_a[group, 0].astype(F32)
            own_bias = total[:, 3 * HD :]
            for j in range(1, KV):
                total = total + recv_a[group, j].astype(F32)
            inv_norm = lax.rsqrt(total[:, 4 * HD - 1 : 4 * HD] / D + EPSILON)
            query = (inv_norm * total[:, 0:HD]).astype(BF16)
            send_q[group] = query
            to_members(1, send_q, recv_q, group)
            if group:
                recv_q[pl.ds(k, 1)] = query[None]
            forget_lane = 2 * (t - 1 + group) + head
            forget_sum = jnp.sum(
                jnp.where(lane == forget_lane, total[:, 3 * HD :], 0.0), axis=1, keepdims=True
            )
            of_head = (lane >= 16) & (lane < 22) & (lax.rem(lane, 2) == head)
            gate_bias = jnp.sum(jnp.where(of_head, own_bias, 0.0), axis=1, keepdims=True)
            gate_in = inv_norm * forget_sum + gate_bias
            log_forget = jnp.minimum(gate_in, 0.0) - jnp.log1p(jnp.exp(-jnp.abs(gate_in)))
            state[group, :, 0:HD] = query.astype(F32)
            for n in (1, 2):
                state[group, :, HD * n : HD * n + HD] = (
                    (inv_norm * total[:, HD * n : HD * n + HD]).astype(BF16).astype(F32)
                )
            state[group, :, 3 * HD :] = jnp.broadcast_to(log_forget, (NEW, 128))

    arrived_at_member(1, recv_q)
    for s in range(SEQS):
        for h in range(HEADS):
            qblk[s, NEW * h : NEW * h + NEW, HD * h : HD * h + HD] = recv_q[2 * s + h].astype(F32)
    for dz in (4, 5, 3, 6, 2, 7, 1, 0):
        z_peer = lax.rem(z + dz, ZS)
        for s in (2 * z_peer, 2 * z_peer + 1):
            scores = jnp.dot(qblk[s].astype(BF16), kt[s], preferred_element_type=F32)
            scores = scores * score_scale + bias[s]
            peak = jnp.maximum(jnp.max(scores, axis=1, keepdims=True), PEAK_FLOOR)
            weights = jnp.exp(scores - peak)
            block_total = jnp.sum(weights, axis=1, keepdims=True)
            block_sum = jnp.dot(weights.astype(BF16), vc[s], preferred_element_type=F32)
            stats = jnp.where(lane8 == 0, peak, jnp.where(lane8 == 1, block_total, last[s]))
            for h in range(HEADS):
                lines = slice(NEW * h, NEW * h + NEW)
                send_b[2 * s + h, :, 0:HD] = block_sum[lines, HD * h : HD * h + HD]
                send_b[2 * s + h, :, HD:] = stats[lines]
        for dy in (2, 1, 3, 0):
            if dz or dy:
                to_owner(2, send_b, recv_b, z_peer * YS + lax.rem(y + dy, YS))
    own_to_owner(2, send_b, recv_b)

    token = lax.broadcasted_iota(jnp.int32, (NEW, 1), 0)

    @pl.when(is_owner)
    def _():
        for group in (1, 0):
            arrived_at_owner(2, recv_b, group)
            past_peak = recv_b[group, 0, :, HD : HD + 1]
            for j in range(1, KV):
                past_peak = jnp.maximum(past_peak, recv_b[group, j, :, HD : HD + 1])
            past_total = jnp.zeros((NEW, 1), F32)
            last_cum = jnp.zeros((NEW, 1), F32)
            past_sum = jnp.zeros((NEW, HD), F32)
            for j in range(KV):
                stats = recv_b[group, j, :, HD:]
                factor = jnp.exp(stats[:, 0:1] - past_peak)
                past_total = past_total + stats[:, 1:2] * factor
                last_cum = last_cum + stats[:, 2:3]
                past_sum = past_sum + recv_b[group, j, :, 0:HD] * factor
            query_wide = state[group, :, 0:HD]
            key_new = state[group, :, HD : 2 * HD]
            value_new = state[group, :, 2 * HD : 3 * HD]
            log_forget = state[group, :, 3 * HD : 3 * HD + 1]
            key_cum = last_cum[0:1, :]
            own_scores = []
            for i in range(NEW):
                key_cum = key_cum + log_forget[i : i + 1, :]
                dots = jnp.sum(query_wide * key_new[i : i + 1, :], axis=1, keepdims=True)
                own_scores.append(jnp.where(token >= i, dots * score_scale - key_cum, NEG_FILL))
            peak_score = past_peak
            for score in own_scores:
                peak_score = jnp.maximum(peak_score, score)
            past_factor = jnp.exp(past_peak - peak_score)
            numerator = past_sum * past_factor
            denominator = past_total * past_factor
            for i, score in enumerate(own_scores):
                weight = jnp.where(token >= i, jnp.exp(score - peak_score), 0.0)
                numerator = numerator + weight.astype(BF16).astype(F32) * value_new[i : i + 1, :]
                denominator = denominator + weight
            attended = (numerator / denominator).astype(BF16)
            send_t[group] = attended
            to_members(3, send_t, recv_t, group)
            if group:
                recv_t[pl.ds(k, 1)] = attended[None]

    loads["wo"].wait()
    arrived_at_member(3, recv_t)
    for s in range(SEQS):
        for h in range(HEADS):
            att[NEW * s : NEW * s + NEW, HD * h : HD * h + HD] = recv_t[2 * s + h].astype(F32)

    send_c[0] = jnp.dot(att[...].astype(BF16), wo[...], preferred_element_type=F32).astype(BF16)
    to_tp(4, send_c.at[0], recv_c)
    recv_c[pl.ds(t, 1)] = send_c[...]
    for name in ("mlp", "wg", "wu"):
        loads[name].wait()
    arrived_tp(4, recv_c)
    attn_out = recv_c[0].astype(F32)
    for j in range(1, TP):
        attn_out = attn_out + recv_c[j].astype(F32)
    middle = (xs[...] + attn_out).astype(BF16).astype(F32)
    xs[...] = middle
    scaled2 = (middle * mlp[...]).astype(BF16)
    squares = jnp.broadcast_to(jnp.sum(middle * middle, axis=1, keepdims=True), (ROWS, 128))
    rough = squares.astype(BF16).astype(F32)
    est[...] = jnp.where(lane64 < 64, rough, squares - rough)

    for s in range(SEQS):
        piece = est[NEW * s : NEW * s + NEW, :].astype(BF16)
        for half in range(2):
            send_e[2 * s + half, :, 0:128] = piece

    def partial_products(dst, at, begin, width, half):
        for n, w in enumerate((wg, wu)):
            part = jnp.dot(scaled2, w[:, begin : begin + width], preferred_element_type=F32)
            for s in range(SEQS):
                dst[2 * s + half, :, at + width * n : at + width * n + width] = part[
                    NEW * s : NEW * s + NEW
                ].astype(BF16)

    for half in range(2):
        partial_products(send_e, 128, CUT * half, FIRST, half)
    for peer in kv_peers:
        to_owner(5, send_e, recv_e, peer)
    own_to_owner(5, send_e, recv_e)
    for half in range(2):
        partial_products(send_l, 0, CUT * half + FIRST, LATE[half] // 2, half)
    for dz, dy in OFFSETS:
        peer = lax.rem(z + dz, ZS) * YS + lax.rem(y + dy, YS)
        half = lax.rem(y + dy, 2)
        for h in range(2):

            @pl.when(half == h)
            def _():
                to_owner(8, send_l, recv_l, peer, LATE[h])

    for h in range(2):

        @pl.when(head == h)
        def _():
            own_to_owner(8, send_l, recv_l, LATE[h])

    def hidden_of(gate, up, inv_norm2):
        gate = inv_norm2 * gate
        return (gate * jax.nn.sigmoid(gate) * (inv_norm2 * up)).astype(BF16)

    @pl.when(is_owner)
    def _():
        for group in (1, 0):
            arrived_at_owner(5, recv_e, group)
            total = recv_e[group, 0].astype(F32)
            for j in range(1, KV):
                total = total + recv_e[group, j].astype(F32)
            inv_norm2 = lax.rsqrt((total[:, 0:1] + total[:, 127:128]) / D + EPSILON)
            hidden = hidden_of(total[:, 128 : 128 + FIRST], total[:, 128 + FIRST :], inv_norm2)
            send_h[group] = hidden
            to_members(6, send_h, recv_h, group)
            if group:
                recv_h[pl.ds(k, 1)] = hidden[None]
            state[group, :, 0:HD] = jnp.broadcast_to(inv_norm2, (NEW, HD))
        for h in range(2):

            @pl.when(head == h)
            def _():
                width = LATE[h]
                for group in (1, 0):
                    arrived_at_owner(8, recv_l, group, width)
                    total = recv_l[group, 0, :, 0:width].astype(F32)
                    for j in range(1, KV):
                        total = total + recv_l[group, j, :, 0:width].astype(F32)
                    hidden = hidden_of(
                        total[:, 0 : width // 2], total[:, width // 2 :], state[group, :, 0:1]
                    )
                    send_m[group, :, 0 : width // 2] = hidden
                    to_members(9, send_m, recv_m, group, width // 2)
                    if group:
                        recv_m[pl.ds(k, 1), :, 0 : width // 2] = hidden[None]

    loads["wd"].wait()
    arrived_at_member(6, recv_h)
    for s in range(SEQS):
        for h in range(2):
            hid[NEW * s : NEW * s + NEW, CUT * h : CUT * h + FIRST] = recv_h[2 * s + h].astype(F32)

    def by_role(enough, sem, name):
        for role, buffer in zip(
            (no_owner, is_owner & (head == 0), is_owner & (head == 1)), enough, strict=True
        ):

            @pl.when(role)
            def _():
                with jax.named_scope(name):
                    wait_bytes(buffer, sem)

    by_role(
        (recv_a.at[0, pl.ds(0, 20)], recv_e.at[0, pl.ds(0, 11)], recv_l.at[0, pl.ds(0, 13)]),
        recv_sem.at[9, 0],
        "recv9",
    )
    for s in range(SEQS):
        for h in range(2):
            begin, width = CUT * h + FIRST, LATE[h] // 2
            hid[NEW * s : NEW * s + NEW, begin : begin + width] = recv_m[
                2 * s + h, :, 0:width
            ].astype(F32)

    send_f[0] = jnp.dot(hid[...].astype(BF16), wd[...], preferred_element_type=F32).astype(BF16)
    to_tp(7, send_f.at[0], recv_f)
    recv_f[pl.ds(t, 1)] = send_f[...]
    arrived_tp(7, recv_f)
    mixed = recv_f[0].astype(F32)
    for j in range(1, TP):
        mixed = mixed + recv_f[j].astype(F32)
    out_ref[...] = (xs[...] + mixed).astype(BF16)

    for phase, buffer in ((4, recv_c), (7, recv_f)):
        wait_bytes(buffer.at[pl.ds(0, TP - 1)], send_sem.at[phase, 0])
    for group, role in ((0, no_owner), (1, is_owner)):

        @pl.when(role)
        def _():
            for phase, buffer in ((0, recv_a), (2, recv_b), (5, recv_e)):
                wait_bytes(buffer.at[0, pl.ds(0, KV - group)], send_sem.at[phase, 0])

    by_role(
        (recv_a.at[:, pl.ds(0, 20)], recv_e.at[0, pl.ds(0, 22)], recv_l.at[0, pl.ds(0, 26)]),
        send_sem.at[8, 0],
        "sent8",
    )

    @pl.when(is_owner)
    def _():
        for group in range(2):
            for phase, buffer in ((1, recv_q), (3, recv_t), (6, recv_h)):
                wait_bytes(buffer.at[pl.ds(0, KV - group)], send_sem.at[phase, group])
        for h in range(2):

            @pl.when(head == h)
            def _():
                for group in range(2):
                    some = recv_m.at[pl.ds(0, KV - group), :, pl.ds(0, LATE[h] // 2)]
                    wait_bytes(some, send_sem.at[9, group])


def on_device(
    tokens,
    mix_gain,
    w_query,
    w_key,
    w_value,
    w_forget,
    forget_bias,
    key_cache,
    value_cache,
    cum_gate,
    lengths,
    w_out,
    mlp_gain,
    w_gate,
    w_up,
    w_down,
):
    in_vmem = [
        tokens,
        mix_gain.reshape(1, WIDTH),
        w_query,
        w_key,
        w_value,
        w_forget.T,
        key_cache,
        value_cache,
        cum_gate,
        w_out,
        mlp_gain.reshape(1, WIDTH),
        w_gate,
        w_up,
        w_down,
    ]
    shapes = [pltpu.VMEM(a.shape, a.dtype) for a in in_vmem]
    shapes[5] = pltpu.VMEM((16, WIDTH), BF16)
    out = pl.pallas_call(
        kernel,
        out_shape=jax.ShapeDtypeStruct((ROWS, WIDTH), BF16),
        in_specs=[pl.BlockSpec(memory_space=pltpu.SMEM)] * 2
        + [pl.BlockSpec(memory_space=pltpu.HBM)] * len(in_vmem),
        out_specs=pl.BlockSpec(memory_space=pltpu.VMEM),
        scratch_shapes=shapes
        + [
            pltpu.VMEM((ROWS, WIDTH), F32),
            pltpu.VMEM((ROWS, 128), F32),
            pltpu.VMEM((SEQS, 8, 2 * HD), F32),
            pltpu.VMEM((SEQS, 2*HD, POS), BF16),
            pltpu.VMEM((SEQS, 8, POS), F32),
            pltpu.VMEM((SEQS, 8, 128), F32),
            pltpu.VMEM((ROWS, 2 * HD), F32),
            pltpu.VMEM((ROWS, FF), F32),
            pltpu.VMEM((2, NEW, 4 * HD), F32),
            pltpu.VMEM((KV, NEW, 4 * HD), BF16),
            pltpu.VMEM((2, KV, NEW, 4 * HD), BF16),
            pltpu.VMEM((2, NEW, HD), BF16),
            pltpu.VMEM((KV, NEW, HD), BF16),
            pltpu.VMEM((KV, NEW, 2 * HD), F32),
            pltpu.VMEM((2, KV, NEW, 2 * HD), F32),
            pltpu.VMEM((2, NEW, HD), BF16),
            pltpu.VMEM((KV, NEW, HD), BF16),
            pltpu.VMEM((1, ROWS, WIDTH), BF16),
            pltpu.VMEM((TP, ROWS, WIDTH), BF16),
            pltpu.VMEM((KV, NEW, EARLY), BF16),
            pltpu.VMEM((2, KV, NEW, EARLY), BF16),
            pltpu.VMEM((KV, NEW, LATE[0]), BF16),
            pltpu.VMEM((2, KV, NEW, LATE[0]), BF16),
            pltpu.VMEM((2, NEW, FIRST), BF16),
            pltpu.VMEM((KV, NEW, FIRST), BF16),
            pltpu.VMEM((2, NEW, LATE[0] // 2), BF16),
            pltpu.VMEM((KV, NEW, LATE[0] // 2), BF16),
            pltpu.VMEM((1, ROWS, WIDTH), BF16),
            pltpu.VMEM((TP, ROWS, WIDTH), BF16),
            pltpu.SemaphoreType.DMA((len(in_vmem),)),
            pltpu.SemaphoreType.DMA((10, 2)),
            pltpu.SemaphoreType.DMA((10, 2)),
        ],
        compiler_params=pltpu.CompilerParams(
            collective_id=0, has_side_effects=True, vmem_limit_bytes=67043328
        ),
    )(lengths, forget_bias, *in_vmem)
    return out.reshape(SEQS, NEW, WIDTH)


def solution(mesh):
    return jax.shard_map(
        on_device,
        mesh=mesh,
        in_specs=(
            P(None, None, "kv"),
            P("kv"),
            P("kv", "tp"),
            P("kv", "tp"),
            P("kv", "tp"),
            P(),
            P("tp"),
            P(None, "kv", "tp"),
            P(None, "kv", "tp"),
            P(None, "tp", "kv"),
            P(),
            P("tp", "kv"),
            P("kv"),
            P("kv", "tp"),
            P("kv", "tp"),
            P("tp", "kv"),
        ),
        out_specs=P(None, None, "kv"),
        check_vma=False,
    )
```

```python
import jax
import jax.numpy as jnp
from jax import lax
from jax.experimental import pallas as pl
from jax.experimental.pallas import tpu as pltpu
from jax.sharding import PartitionSpec as P

D = 4096
EPSILON = 1e-06
NEG_FILL = -1e30
PEAK_FLOOR = -1e29
SEQS = 16
NEW = 4
ROWS = SEQS * NEW
HEADS = 2
HD = 128
WIDTH = 128
POS = 512
FF = 1408
CUT = 768
FIRST = 384
EARLY = 128 + 2 * FIRST
LATE = (2 * (CUT - FIRST), 2 * (FF - CUT - FIRST))
KV = 32
TP = 8
ZS, YS = 8, 4
F32 = jnp.float32
BF16 = jnp.bfloat16
MESH = pl.DeviceIdType.MESH


OFFSETS = sorted(
    ((dz, dy) for dz in range(ZS) for dy in range(YS) if dz or dy),
    key=lambda o: -(min(o[0], ZS - o[0]) + min(o[1], YS - o[1])),
)


def kernel(
    lengths_ref,
    bias_ref,
    tokens_hbm,
    mix_hbm,
    wq_hbm,
    wk_hbm,
    wv_hbm,
    wf_hbm,
    kc_hbm,
    vc_hbm,
    cg_hbm,
    wo_hbm,
    mlp_hbm,
    wg_hbm,
    wu_hbm,
    wd_hbm,
    out_ref,
    tok,
    mix,
    wq,
    wk,
    wv,
    wf,
    kc,
    vc,
    cg,
    wo,
    mlp,
    wg,
    wu,
    wd,
    xs,
    est,
    qblk,
    kt,
    bias,
    last,
    att,
    hid,
    state,
    send_a,
    recv_a,
    send_k,
    recv_k,
    send_q,
    recv_q,
    send_b,
    recv_b,
    send_t,
    recv_t,
    send_c,
    recv_c,
    send_e,
    recv_e,
    send_l,
    recv_l,
    send_h,
    recv_h,
    send_m,
    recv_m,
    send_f,
    recv_f,
    in_sem,
    send_sem,
    recv_sem,
):
    k = lax.axis_index("kv")
    t = lax.axis_index("tp")
    z, y = k // YS, lax.rem(k, YS)
    head = lax.rem(k, 2)
    mine = k // 2

    loads = {}
    sources = dict(
        tok=(tokens_hbm, tok),
        mix=(mix_hbm, mix),
        wq=(wq_hbm, wq),
        wk=(wk_hbm, wk),
        wv=(wv_hbm, wv),
        wf=(wf_hbm.at[:, pl.ds(pl.multiple_of(k * WIDTH, WIDTH), WIDTH)], wf),
        kc=(kc_hbm, kc),
        vc=(vc_hbm, vc),
        cg=(cg_hbm, cg),
        wo=(wo_hbm, wo),
        mlp=(mlp_hbm, mlp),
        wg=(wg_hbm, wg),
        wu=(wu_hbm, wu),
        wd=(wd_hbm, wd),
    )
    kv_peers = [lax.rem(z + dz, ZS) * YS + lax.rem(y + dy, YS) for dz, dy in OFFSETS]
    tp_peers = [lax.rem(t + d, TP) for d in (4, 5, 3, 2, 6, 7, 1)]
    core = lax.rem(t, 2)
    owner_t = t + 1 - core
    is_owner = core == 1
    no_owner = core == 0

    barrier = pltpu.get_barrier_semaphore()

    def greet(kv, tp):
        pl.semaphore_signal(barrier, inc=1, device_id=(kv, tp), device_id_type=MESH)

    for peer in kv_peers:
        greet(peer, owner_t)

    @pl.when(is_owner)
    def _():
        for peer in kv_peers:
            greet(peer, t - 1)

    for peer in tp_peers:
        greet(k, peer)

    for n, (name, (src, dst)) in enumerate(sources.items()):
        loads[name] = pltpu.make_async_copy(src, dst, in_sem.at[n])
        loads[name].start()

    def send(src, dst, sent, received, kv, tp):
        pltpu.make_async_remote_copy(
            src_ref=src,
            dst_ref=dst,
            send_sem=sent,
            recv_sem=received,
            device_id=(kv, tp),
            device_id_type=MESH,
        ).start()

    def lanes(ref, width, begin=0):
        return ref if width is None else ref.at[:, pl.ds(begin, width)]

    def to_owner(phase, src, dst, peer, width=None, begin=0):
        send(
            lanes(src.at[peer], width, begin),
            lanes(dst.at[core, k], width, begin),
            send_sem.at[phase, 0],
            recv_sem.at[phase, core],
            peer,
            owner_t,
        )

    def own_to_owner(phase, src, dst, width=None, begin=0):
        @pl.when(no_owner)
        def _():
            to_owner(phase, src, dst, k, width, begin)

        @pl.when(is_owner)
        def _():
            dst[1, pl.ds(k, 1)] = src[pl.ds(k, 1)]

    def to_members(phase, src, dst, group, width=None):
        peers = kv_peers if group else kv_peers + [k]
        for peer in peers:
            send(
                lanes(src.at[group], width),
                lanes(dst.at[k], width),
                send_sem.at[phase, group],
                recv_sem.at[phase, 0],
                peer,
                t - 1 + group,
            )

    def to_tp(phase, src, dst):
        for peer in tp_peers:
            send(src, dst.at[t], send_sem.at[phase, 0], recv_sem.at[phase, 0], k, peer)

    def wait_bytes(ref, sem):
        pltpu.make_async_copy(ref, ref, sem).wait()

    def arrived_at_owner(phase, dst, group, width=None, begin=0):
        count = KV - group
        some = dst.at[group, pl.ds(0, count)]
        if width is not None:
            some = dst.at[group, pl.ds(0, count), :, pl.ds(begin, width)]
        with jax.named_scope("own%d_%d" % (phase, group)):
            wait_bytes(some, recv_sem.at[phase, group])

    def arrived_at_member(phase, dst):
        for group, role in ((0, no_owner), (1, is_owner)):

            @pl.when(role)
            def _():
                with jax.named_scope("recv%d" % phase):
                    wait_bytes(dst.at[pl.ds(0, KV - group)], recv_sem.at[phase, 0])

    def arrived_tp(phase, dst):
        with jax.named_scope("recv%d" % phase):
            wait_bytes(dst.at[pl.ds(0, TP - 1)], recv_sem.at[phase, 0])

    for name in ("tok", "mix"):
        loads[name].wait()
    for s in range(SEQS):
        xs[NEW * s : NEW * s + NEW, :] = tok[s].astype(F32)
    x = xs[...]
    scaled = (x * mix[...]).astype(BF16)
    est[...] = jnp.broadcast_to(jnp.sum(x * x, axis=1, keepdims=True), (ROWS, 128))
    loads["wf"].wait()
    est[:, 0:16] = lax.dot_general(
        scaled, wf[...], (((1,), (1,)), ((), ())), preferred_element_type=F32
    )
    lane64 = lax.broadcasted_iota(jnp.int32, (ROWS, 128), 1)
    bias_all = jnp.where(lax.rem(lane64, 2) == 0, bias_ref[0], bias_ref[1])
    high = bias_all.astype(BF16).astype(F32)
    middle_part = (bias_all - high).astype(BF16).astype(F32)
    low = bias_all - high - middle_part
    parts = jnp.where(lane64 < 18, high, jnp.where(lane64 < 20, middle_part, low))
    est[...] = jnp.where((lane64 >= 16) & (lane64 < 22), parts, est[...])
    def project(name, w, dst, at):
        loads[name].wait()
        part = jnp.dot(scaled, w[...], preferred_element_type=F32)
        for s in range(SEQS):
            for h in range(HEADS):
                dst[2 * s + h, :, at : at + HD] = part[
                    NEW * s : NEW * s + NEW, HD * h : HD * h + HD
                ].astype(BF16)

    project("wq", wq, send_a, 0)
    for s in range(SEQS):
        piece = est[NEW * s : NEW * s + NEW, :].astype(BF16)
        for h in range(HEADS):
            send_a[2 * s + h, :, HD:] = piece
    with jax.named_scope("barrier"):
        pl.semaphore_wait(barrier, KV - 1 + TP - 1 + (KV - 1) * core)
    for peer in kv_peers:
        to_owner(0, send_a, recv_a, peer)
    own_to_owner(0, send_a, recv_a)

    qblk[...] = jnp.zeros(qblk.shape, F32)
    for name in ("kc", "vc", "cg"):
        loads[name].wait()
    score_scale = HD**-0.5
    position = k * POS + lax.broadcasted_iota(jnp.int32, (8, POS), 1)
    row8 = lax.broadcasted_iota(jnp.int32, (8, POS), 0)
    lane8 = lax.broadcasted_iota(jnp.int32, (8, 128), 1)
    for s in range(SEQS):
        length = lengths_ref[s]
        both = cg[s]
        cum = jnp.where(row8 < NEW, both[0:1, :], both[1:2, :])
        bias[s] = jnp.where(position < length, -cum, NEG_FILL)
        at_last = jnp.sum(jnp.where(position == length - 1, cum, 0.0), axis=1, keepdims=True)
        high = at_last.astype(BF16).astype(F32)
        middle_part = (at_last - high).astype(BF16).astype(F32)
        low = at_last - high - middle_part
        last[s] = jnp.where(
            lane8 == 3, high, jnp.where(lane8 == 4, middle_part, jnp.where(lane8 == 5, low, 0.0))
        )
    for s in range(SEQS):
        kt[s] = kc[s].T
    project("wk", wk, send_k, 0)
    project("wv", wv, send_k, HD)
    for peer in kv_peers:
        to_owner(10, send_k, recv_k, peer)
    own_to_owner(10, send_k, recv_k)

    lane = lax.broadcasted_iota(jnp.int32, (NEW, 128), 1)

    @pl.when(is_owner)
    def _():
        for group in (1, 0):
            arrived_at_owner(0, recv_a, group)
            total = recv_a[group, 0].astype(F32)
            own_bias = total[:, HD:]
            for j in range(1, KV):
                total = total + recv_a[group, j].astype(F32)
            inv_norm = lax.rsqrt(total[:, 2 * HD - 1 : 2 * HD] / D + EPSILON)
            query = (inv_norm * total[:, 0:HD]).astype(BF16)
            send_q[group] = query
            to_members(1, send_q, recv_q, group)
            if group:
                recv_q[pl.ds(k, 1)] = query[None]
            forget_lane = 2 * (t - 1 + group) + head
            forget_sum = jnp.sum(
                jnp.where(lane == forget_lane, total[:, HD:], 0.0), axis=1, keepdims=True
            )
            of_head = (lane >= 16) & (lane < 22) & (lax.rem(lane, 2) == head)
            gate_bias = jnp.sum(jnp.where(of_head, own_bias, 0.0), axis=1, keepdims=True)
            gate_in = inv_norm * forget_sum + gate_bias
            log_forget = jnp.minimum(gate_in, 0.0) - jnp.log1p(jnp.exp(-jnp.abs(gate_in)))
            state[group, :, 0:HD] = query.astype(F32)
            state[group, :, 3 * HD : 4 * HD] = jnp.broadcast_to(log_forget, (NEW, HD))
            state[group, :, 4 * HD :] = jnp.broadcast_to(inv_norm, (NEW, HD))

    arrived_at_member(1, recv_q)
    for s in range(SEQS):
        for h in range(HEADS):
            qblk[s, NEW * h : NEW * h + NEW, HD * h : HD * h + HD] = recv_q[2 * s + h].astype(F32)
    for dz in (4, 5, 3, 6, 2, 7, 1, 0):
        z_peer = lax.rem(z + dz, ZS)
        for s in (2 * z_peer, 2 * z_peer + 1):
            scores = jnp.dot(qblk[s].astype(BF16), kt[s], preferred_element_type=F32)
            scores = scores * score_scale + bias[s]
            peak = jnp.maximum(jnp.max(scores, axis=1, keepdims=True), PEAK_FLOOR)
            peak = peak.astype(BF16).astype(F32)
            weights = jnp.exp(scores - peak)
            block_total = jnp.sum(weights, axis=1, keepdims=True)
            block_sum = jnp.dot(weights.astype(BF16), vc[s], preferred_element_type=F32)
            high = block_total.astype(BF16).astype(F32)
            stats = jnp.where(
                lane8 == 0,
                peak,
                jnp.where(lane8 == 1, high, jnp.where(lane8 == 2, block_total - high, last[s])),
            )
            for h in range(HEADS):
                lines = slice(NEW * h, NEW * h + NEW)
                send_b[2 * s + h, :, 0:HD] = block_sum[lines, HD * h : HD * h + HD].astype(BF16)
                send_b[2 * s + h, :, HD:] = stats[lines].astype(BF16)
        for dy in (2, 1, 3, 0):
            if dz or dy:
                to_owner(2, send_b, recv_b, z_peer * YS + lax.rem(y + dy, YS))
    own_to_owner(2, send_b, recv_b)

    token = lax.broadcasted_iota(jnp.int32, (NEW, 1), 0)

    @pl.when(is_owner)
    def _():
        for group in (1, 0):
            arrived_at_owner(10, recv_k, group)
            total = recv_k[group, 0].astype(F32)
            for j in range(1, KV):
                total = total + recv_k[group, j].astype(F32)
            state[group, :, HD : 3 * HD] = (
                (state[group, :, 4 * HD : 4 * HD + 1] * total).astype(BF16).astype(F32)
            )
        for group in (1, 0):
            arrived_at_owner(2, recv_b, group)
            past_peak = recv_b[group, 0, :, HD:].astype(F32)
            for j in range(1, KV):
                past_peak = jnp.maximum(past_peak, recv_b[group, j, :, HD:].astype(F32))
            past_peak = past_peak[:, 0:1]
            weighted = jnp.zeros((NEW, HD), F32)
            gates = jnp.zeros((NEW, HD), F32)
            past_sum = jnp.zeros((NEW, HD), F32)
            for j in range(KV):
                stats = recv_b[group, j, :, HD:].astype(F32)
                factor = jnp.exp(stats[:, 0:1] - past_peak)
                weighted = weighted + stats * factor
                gates = gates + stats
                past_sum = past_sum + recv_b[group, j, :, 0:HD].astype(F32) * factor
            past_total = weighted[:, 1:2] + weighted[:, 2:3]
            last_cum = gates[:, 3:4] + gates[:, 4:5] + gates[:, 5:6]
            query_wide = state[group, :, 0:HD]
            key_new = state[group, :, HD : 2 * HD]
            value_new = state[group, :, 2 * HD : 3 * HD]
            log_forget = state[group, :, 3 * HD : 3 * HD + 1]
            key_cum = last_cum[0:1, :]
            own_scores = []
            for i in range(NEW):
                key_cum = key_cum + log_forget[i : i + 1, :]
                dots = jnp.sum(query_wide * key_new[i : i + 1, :], axis=1, keepdims=True)
                own_scores.append(jnp.where(token >= i, dots * score_scale - key_cum, NEG_FILL))
            peak_score = past_peak
            for score in own_scores:
                peak_score = jnp.maximum(peak_score, score)
            past_factor = jnp.exp(past_peak - peak_score)
            numerator = past_sum * past_factor
            denominator = past_total * past_factor
            for i, score in enumerate(own_scores):
                weight = jnp.where(token >= i, jnp.exp(score - peak_score), 0.0)
                numerator = numerator + weight.astype(BF16).astype(F32) * value_new[i : i + 1, :]
                denominator = denominator + weight
            attended = (numerator / denominator).astype(BF16)
            send_t[group] = attended
            to_members(3, send_t, recv_t, group)
            if group:
                recv_t[pl.ds(k, 1)] = attended[None]

    loads["wo"].wait()
    arrived_at_member(3, recv_t)
    for s in range(SEQS):
        for h in range(HEADS):
            att[NEW * s : NEW * s + NEW, HD * h : HD * h + HD] = recv_t[2 * s + h].astype(F32)

    send_c[0] = jnp.dot(att[...].astype(BF16), wo[...], preferred_element_type=F32).astype(BF16)
    to_tp(4, send_c.at[0], recv_c)
    recv_c[pl.ds(t, 1)] = send_c[...]
    for name in ("mlp", "wg", "wu"):
        loads[name].wait()
    arrived_tp(4, recv_c)
    attn_out = recv_c[0].astype(F32)
    for j in range(1, TP):
        attn_out = attn_out + recv_c[j].astype(F32)
    middle = (xs[...] + attn_out).astype(BF16).astype(F32)
    xs[...] = middle
    scaled2 = (middle * mlp[...]).astype(BF16)

    @pl.when(is_owner)
    def _():
        squares = jnp.broadcast_to(jnp.sum(middle * middle, axis=1, keepdims=True), (ROWS, 128))
        rough = squares.astype(BF16).astype(F32)
        both_parts = jnp.where(lane64 < 64, rough, squares - rough)
        for s in range(SEQS):
            piece = both_parts[NEW * s : NEW * s + NEW, :].astype(BF16)
            for half in range(2):
                send_e[2 * s + half, :, 0:128] = piece

    def partial_products(dst, at, begin, width, half):
        for n, w in enumerate((wg, wu)):
            part = jnp.dot(scaled2, w[:, begin : begin + width], preferred_element_type=F32)
            for s in range(SEQS):
                dst[2 * s + half, :, at + width * n : at + width * n + width] = part[
                    NEW * s : NEW * s + NEW
                ].astype(BF16)

    for half in range(2):
        partial_products(send_e, 128, CUT * half, FIRST, half)

    @pl.when(is_owner)
    def _():
        for peer in kv_peers:
            to_owner(5, send_e, recv_e, peer)

    @pl.when(no_owner)
    def _():
        for peer in kv_peers:
            to_owner(5, send_e, recv_e, peer, 2 * FIRST, 128)

    own_to_owner(5, send_e, recv_e, 2 * FIRST, 128)
    for half in range(2):
        partial_products(send_l, 0, CUT * half + FIRST, LATE[half] // 2, half)
    for dz, dy in OFFSETS:
        peer = lax.rem(z + dz, ZS) * YS + lax.rem(y + dy, YS)
        half = lax.rem(y + dy, 2)
        for h in range(2):

            @pl.when(half == h)
            def _():
                to_owner(8, send_l, recv_l, peer, LATE[h])

    for h in range(2):

        @pl.when(head == h)
        def _():
            own_to_owner(8, send_l, recv_l, LATE[h])

    def hidden_of(gate, up, inv_norm2):
        gate = inv_norm2 * gate
        return (gate * jax.nn.sigmoid(gate) * (inv_norm2 * up)).astype(BF16)

    @pl.when(is_owner)
    def _():
        for group in (1, 0):
            if group:
                arrived_at_owner(5, recv_e, 1)
                total = recv_e[1, 0, :, 0:128].astype(F32)
                for j in range(1, KV):
                    total = total + recv_e[1, j, :, 0:128].astype(F32)
                inv_norm2 = lax.rsqrt((total[:, 0:1] + total[:, 127:128]) / D + EPSILON)
            else:
                arrived_at_owner(5, recv_e, 0, 2 * FIRST, 128)
            total = recv_e[group, 0, :, 128:].astype(F32)
            for j in range(1, KV):
                total = total + recv_e[group, j, :, 128:].astype(F32)
            hidden = hidden_of(total[:, 0:FIRST], total[:, FIRST:], inv_norm2)
            send_h[group] = hidden
            to_members(6, send_h, recv_h, group)
            if group:
                recv_h[pl.ds(k, 1)] = hidden[None]
            state[group, :, 0:HD] = jnp.broadcast_to(inv_norm2, (NEW, HD))
        for h in range(2):

            @pl.when(head == h)
            def _():
                width = LATE[h]
                for group in (1, 0):
                    arrived_at_owner(8, recv_l, group, width)
                    total = recv_l[group, 0, :, 0:width].astype(F32)
                    for j in range(1, KV):
                        total = total + recv_l[group, j, :, 0:width].astype(F32)
                    hidden = hidden_of(
                        total[:, 0 : width // 2], total[:, width // 2 :], state[group, :, 0:1]
                    )
                    send_m[group, :, 0 : width // 2] = hidden
                    to_members(9, send_m, recv_m, group, width // 2)
                    if group:
                        recv_m[pl.ds(k, 1), :, 0 : width // 2] = hidden[None]

    loads["wd"].wait()
    arrived_at_member(6, recv_h)
    for s in range(SEQS):
        for h in range(2):
            hid[NEW * s : NEW * s + NEW, CUT * h : CUT * h + FIRST] = recv_h[2 * s + h].astype(F32)

    def by_role(enough, sem, name):
        for role, buffer in zip(
            (no_owner, is_owner & (head == 0), is_owner & (head == 1)), enough, strict=True
        ):

            @pl.when(role)
            def _():
                with jax.named_scope(name):
                    wait_bytes(buffer, sem)

    by_role(
        (kt.at[0, pl.ds(0, 80)], recv_e.at[0, pl.ds(0, 11)], recv_l.at[0, pl.ds(0, 13)]),
        recv_sem.at[9, 0],
        "recv9",
    )
    for s in range(SEQS):
        for h in range(2):
            begin, width = CUT * h + FIRST, LATE[h] // 2
            hid[NEW * s : NEW * s + NEW, begin : begin + width] = recv_m[
                2 * s + h, :, 0:width
            ].astype(F32)

    send_f[0] = jnp.dot(hid[...].astype(BF16), wd[...], preferred_element_type=F32).astype(BF16)
    to_tp(7, send_f.at[0], recv_f)
    recv_f[pl.ds(t, 1)] = send_f[...]
    arrived_tp(7, recv_f)
    mixed = recv_f[0].astype(F32)
    for j in range(1, TP):
        mixed = mixed + recv_f[j].astype(F32)
    out_ref[...] = (xs[...] + mixed).astype(BF16)

    for phase, buffer in ((4, recv_c), (7, recv_f)):
        wait_bytes(buffer.at[pl.ds(0, TP - 1)], send_sem.at[phase, 0])
    for group, role in ((0, no_owner), (1, is_owner)):

        @pl.when(role)
        def _():
            for phase, buffer in ((0, recv_a), (2, recv_b), (10, recv_k)):
                wait_bytes(buffer.at[0, pl.ds(0, KV - group)], send_sem.at[phase, 0])
            first = 128 * (1 - group)
            some = recv_e.at[0, pl.ds(0, KV - group), :, pl.ds(first, EARLY - first)]
            wait_bytes(some, send_sem.at[5, 0])

    by_role(
        (kt.at[0, pl.ds(0, 160)], recv_e.at[0, pl.ds(0, 22)], recv_l.at[0, pl.ds(0, 26)]),
        send_sem.at[8, 0],
        "sent8",
    )

    @pl.when(is_owner)
    def _():
        for group in range(2):
            for phase, buffer in ((1, recv_q), (3, recv_t), (6, recv_h)):
                wait_bytes(buffer.at[pl.ds(0, KV - group)], send_sem.at[phase, group])
        for h in range(2):

            @pl.when(head == h)
            def _():
                for group in range(2):
                    some = recv_m.at[pl.ds(0, KV - group), :, pl.ds(0, LATE[h] // 2)]
                    wait_bytes(some, send_sem.at[9, group])


def on_device(
    tokens,
    mix_gain,
    w_query,
    w_key,
    w_value,
    w_forget,
    forget_bias,
    key_cache,
    value_cache,
    cum_gate,
    lengths,
    w_out,
    mlp_gain,
    w_gate,
    w_up,
    w_down,
):
    in_vmem = [
        tokens,
        mix_gain.reshape(1, WIDTH),
        w_query,
        w_key,
        w_value,
        w_forget.T,
        key_cache,
        value_cache,
        cum_gate,
        w_out,
        mlp_gain.reshape(1, WIDTH),
        w_gate,
        w_up,
        w_down,
    ]
    shapes = [pltpu.VMEM(a.shape, a.dtype) for a in in_vmem]
    shapes[5] = pltpu.VMEM((16, WIDTH), BF16)
    out = pl.pallas_call(
        kernel,
        out_shape=jax.ShapeDtypeStruct((ROWS, WIDTH), BF16),
        in_specs=[pl.BlockSpec(memory_space=pltpu.SMEM)] * 2
        + [pl.BlockSpec(memory_space=pltpu.HBM)] * len(in_vmem),
        out_specs=pl.BlockSpec(memory_space=pltpu.VMEM),
        scratch_shapes=shapes
        + [
            pltpu.VMEM((ROWS, WIDTH), F32),
            pltpu.VMEM((ROWS, 128), F32),
            pltpu.VMEM((SEQS, 8, 2 * HD), F32),
            pltpu.VMEM((SEQS, 2*HD, POS), BF16),
            pltpu.VMEM((SEQS, 8, POS), F32),
            pltpu.VMEM((SEQS, 8, 128), F32),
            pltpu.VMEM((ROWS, 2 * HD), F32),
            pltpu.VMEM((ROWS, FF), F32),
            pltpu.VMEM((2, NEW, 5 * HD), F32),
            pltpu.VMEM((KV, NEW, 2 * HD), BF16),
            pltpu.VMEM((2, KV, NEW, 2 * HD), BF16),
            pltpu.VMEM((KV, NEW, 2 * HD), BF16),
            pltpu.VMEM((2, KV, NEW, 2 * HD), BF16),
            pltpu.VMEM((2, NEW, HD), BF16),
            pltpu.VMEM((KV, NEW, HD), BF16),
            pltpu.VMEM((KV, NEW, 2 * HD), BF16),
            pltpu.VMEM((2, KV, NEW, 2 * HD), BF16),
            pltpu.VMEM((2, NEW, HD), BF16),
            pltpu.VMEM((KV, NEW, HD), BF16),
            pltpu.VMEM((1, ROWS, WIDTH), BF16),
            pltpu.VMEM((TP, ROWS, WIDTH), BF16),
            pltpu.VMEM((KV, NEW, EARLY), BF16),
            pltpu.VMEM((2, KV, NEW, EARLY), BF16),
            pltpu.VMEM((KV, NEW, LATE[0]), BF16),
            pltpu.VMEM((2, KV, NEW, LATE[0]), BF16),
            pltpu.VMEM((2, NEW, FIRST), BF16),
            pltpu.VMEM((KV, NEW, FIRST), BF16),
            pltpu.VMEM((2, NEW, LATE[0] // 2), BF16),
            pltpu.VMEM((KV, NEW, LATE[0] // 2), BF16),
            pltpu.VMEM((1, ROWS, WIDTH), BF16),
            pltpu.VMEM((TP, ROWS, WIDTH), BF16),
            pltpu.SemaphoreType.DMA((len(in_vmem),)),
            pltpu.SemaphoreType.DMA((11, 2)),
            pltpu.SemaphoreType.DMA((11, 2)),
        ],
        compiler_params=pltpu.CompilerParams(
            collective_id=0, has_side_effects=True, vmem_limit_bytes=67043328
        ),
    )(lengths, forget_bias, *in_vmem)
    return out.reshape(SEQS, NEW, WIDTH)


def solution(mesh):
    return jax.shard_map(
        on_device,
        mesh=mesh,
        in_specs=(
            P(None, None, "kv"),
            P("kv"),
            P("kv", "tp"),
            P("kv", "tp"),
            P("kv", "tp"),
            P(),
            P("tp"),
            P(None, "kv", "tp"),
            P(None, "kv", "tp"),
            P(None, "tp", "kv"),
            P(),
            P("tp", "kv"),
            P("kv"),
            P("kv", "tp"),
            P("kv", "tp"),
            P("tp", "kv"),
        ),
        out_specs=P(None, None, "kv"),
        check_vma=False,
    )
```

```python
import jax
import jax.numpy as jnp
from jax import lax
from jax.experimental import pallas as pl
from jax.experimental.pallas import tpu as pltpu
from jax.sharding import PartitionSpec as P

D = 4096
EPSILON = 1e-06
NEG_FILL = -1e30
PEAK_FLOOR = -1e29
SEQS = 16
NEW = 4
ROWS = SEQS * NEW
HEADS = 2
HD = 128
WIDTH = 128
POS = 512
FF = 1408
CUT = 768
FIRST = 512
EARLY = 128 + 2 * FIRST
LATE = (2 * (CUT - FIRST), 2 * (FF - CUT - FIRST))
KV = 32
TP = 8
ZS, YS = 8, 4
F32 = jnp.float32
BF16 = jnp.bfloat16
MESH = pl.DeviceIdType.MESH


OFFSETS = sorted(
    ((dz, dy) for dz in range(ZS) for dy in range(YS) if dz or dy),
    key=lambda o: -(min(o[0], ZS - o[0]) + min(o[1], YS - o[1])),
)


def kernel(
    lengths_hbm,
    bias_hbm,
    tokens_hbm,
    mix_hbm,
    wq_hbm,
    wk_hbm,
    wv_hbm,
    wf_hbm,
    kc_hbm,
    vc_hbm,
    cg_hbm,
    wo_hbm,
    mlp_hbm,
    wg_hbm,
    wu_hbm,
    wd_hbm,
    out_ref,
    lengths_ref,
    bias_ref,
    tok,
    mix,
    wq,
    wk,
    wv,
    wf,
    kc,
    vc,
    cg,
    wo,
    mlp,
    wg,
    wu,
    wd,
    xs,
    est,
    qblk,
    kt,
    bias,
    last,
    att,
    hid,
    state,
    blocks,
    send_a,
    recv_a,
    send_k,
    recv_k,
    send_q,
    recv_q,
    send_b,
    recv_b,
    send_t,
    recv_t,
    send_c,
    recv_c,
    send_e,
    recv_e,
    send_l,
    recv_l,
    send_h,
    recv_h,
    send_m,
    recv_m,
    send_f,
    recv_f,
    in_sem,
    send_sem,
    recv_sem,
):
    k = lax.axis_index("kv")
    t = lax.axis_index("tp")
    z, y = k // YS, lax.rem(k, YS)
    head = lax.rem(k, 2)
    mine = k // 2

    loads = {}
    sources = dict(
        tok=(tokens_hbm, tok),
        mix=(mix_hbm, mix),
        bias=(bias_hbm, bias_ref),
        wq=(wq_hbm, wq),
        wf=(wf_hbm.at[:, pl.ds(pl.multiple_of(k * WIDTH, WIDTH), WIDTH)], wf),
        lengths=(lengths_hbm, lengths_ref),
        wk=(wk_hbm, wk),
        wv=(wv_hbm, wv),
        kc=(kc_hbm, kc),
        vc=(vc_hbm, vc),
        cg=(cg_hbm, cg),
        wo=(wo_hbm, wo),
        mlp=(mlp_hbm, mlp),
        wg=(wg_hbm, wg),
        wu=(wu_hbm, wu),
        wd=(wd_hbm, wd),
    )
    kv_peers = [lax.rem(z + dz, ZS) * YS + lax.rem(y + dy, YS) for dz, dy in OFFSETS]
    tp_peers = [lax.rem(t + d, TP) for d in (4, 5, 3, 2, 6, 7, 1)]
    core = lax.rem(t, 2)
    owner_t = t + 1 - core
    is_owner = core == 1
    no_owner = core == 0

    barrier = pltpu.get_barrier_semaphore()

    def greet(kv, tp):
        pl.semaphore_signal(barrier, inc=1, device_id=(kv, tp), device_id_type=MESH)

    for peer in kv_peers:
        greet(peer, owner_t)

    @pl.when(is_owner)
    def _():
        for peer in kv_peers:
            greet(peer, t - 1)

    for peer in tp_peers:
        greet(k, peer)

    for n, (name, (src, dst)) in enumerate(sources.items()):
        loads[name] = pltpu.make_async_copy(src, dst, in_sem.at[n])
        loads[name].start()

    def send(src, dst, sent, received, kv, tp):
        pltpu.make_async_remote_copy(
            src_ref=src,
            dst_ref=dst,
            send_sem=sent,
            recv_sem=received,
            device_id=(kv, tp),
            device_id_type=MESH,
        ).start()

    def lanes(ref, width, begin=0):
        return ref if width is None else ref.at[:, pl.ds(begin, width)]

    def to_owner(phase, src, dst, peer, width=None, begin=0):
        send(
            lanes(src.at[peer], width, begin),
            lanes(dst.at[core, k], width, begin),
            send_sem.at[phase, 0],
            recv_sem.at[phase, core],
            peer,
            owner_t,
        )

    def own_to_owner(phase, src, dst, width=None, begin=0):
        @pl.when(no_owner)
        def _():
            to_owner(phase, src, dst, k, width, begin)

        @pl.when(is_owner)
        def _():
            dst[1, pl.ds(k, 1)] = src[pl.ds(k, 1)]

    def to_members(phase, src, dst, group, width=None):
        peers = kv_peers if group else kv_peers + [k]
        for peer in peers:
            send(
                lanes(src.at[group], width),
                lanes(dst.at[k], width),
                send_sem.at[phase, group],
                recv_sem.at[phase, 0],
                peer,
                t - 1 + group,
            )

    def to_tp(phase, src, dst):
        for peer in tp_peers:
            send(src, dst.at[t], send_sem.at[phase, 0], recv_sem.at[phase, 0], k, peer)

    def wait_bytes(ref, sem):
        pltpu.make_async_copy(ref, ref, sem).wait()

    def arrived_at_owner(phase, dst, group, width=None, begin=0):
        count = KV - group
        some = dst.at[group, pl.ds(0, count)]
        if width is not None:
            some = dst.at[group, pl.ds(0, count), :, pl.ds(begin, width)]
        with jax.named_scope("own%d_%d" % (phase, group)):
            wait_bytes(some, recv_sem.at[phase, group])

    def arrived_at_member(phase, dst):
        for group, role in ((0, no_owner), (1, is_owner)):

            @pl.when(role)
            def _():
                with jax.named_scope("recv%d" % phase):
                    wait_bytes(dst.at[pl.ds(0, KV - group)], recv_sem.at[phase, 0])

    def arrived_tp(phase, dst):
        with jax.named_scope("recv%d" % phase):
            wait_bytes(dst.at[pl.ds(0, TP - 1)], recv_sem.at[phase, 0])

    for name in ("tok", "mix"):
        loads[name].wait()
    for s in range(SEQS):
        xs[NEW * s : NEW * s + NEW, :] = tok[s].astype(F32)
    x = xs[...]
    scaled = (x * mix[...]).astype(BF16)
    est[...] = jnp.broadcast_to(jnp.sum(x * x, axis=1, keepdims=True), (ROWS, 128))
    loads["wf"].wait()
    est[:, 0:16] = lax.dot_general(
        scaled, wf[...], (((1,), (1,)), ((), ())), preferred_element_type=F32
    )
    loads["bias"].wait()
    lane64 = lax.broadcasted_iota(jnp.int32, (ROWS, 128), 1)
    bias_all = jnp.where(lax.rem(lane64, 2) == 0, bias_ref[0], bias_ref[1])
    high = bias_all.astype(BF16).astype(F32)
    middle_part = (bias_all - high).astype(BF16).astype(F32)
    low = bias_all - high - middle_part
    parts = jnp.where(lane64 < 18, high, jnp.where(lane64 < 20, middle_part, low))
    est[...] = jnp.where((lane64 >= 16) & (lane64 < 22), parts, est[...])
    def project(name, w, dst, at):
        loads[name].wait()
        part = jnp.dot(scaled, w[...], preferred_element_type=F32)
        for s in range(SEQS):
            for h in range(HEADS):
                dst[2 * s + h, :, at : at + HD] = part[
                    NEW * s : NEW * s + NEW, HD * h : HD * h + HD
                ].astype(BF16)

    project("wq", wq, send_a, 0)
    for s in range(SEQS):
        piece = est[NEW * s : NEW * s + NEW, :].astype(BF16)
        for h in range(HEADS):
            send_a[2 * s + h, :, HD:] = piece
    with jax.named_scope("barrier"):
        pl.semaphore_wait(barrier, KV - 1 + TP - 1 + (KV - 1) * core)
    for peer in kv_peers:
        to_owner(0, send_a, recv_a, peer)
    own_to_owner(0, send_a, recv_a)

    qblk[...] = jnp.zeros(qblk.shape, F32)
    for name in ("kc", "vc", "cg", "lengths"):
        loads[name].wait()
    score_scale = HD**-0.5
    position = k * POS + lax.broadcasted_iota(jnp.int32, (8, POS), 1)
    row8 = lax.broadcasted_iota(jnp.int32, (8, POS), 0)
    lane8 = lax.broadcasted_iota(jnp.int32, (8, 128), 1)
    for s in range(SEQS):
        length = lengths_ref[s]
        both = cg[s]
        cum = jnp.where(row8 < NEW, both[0:1, :], both[1:2, :])
        bias[s] = jnp.where(position < length, -cum, NEG_FILL)
        at_last = jnp.sum(jnp.where(position == length - 1, cum, 0.0), axis=1, keepdims=True)
        high = at_last.astype(BF16).astype(F32)
        middle_part = (at_last - high).astype(BF16).astype(F32)
        low = at_last - high - middle_part
        last[s] = jnp.where(
            lane8 == 3, high, jnp.where(lane8 == 4, middle_part, jnp.where(lane8 == 5, low, 0.0))
        )
    for s in range(SEQS):
        kt[s] = kc[s].T
    project("wk", wk, send_k, 0)
    project("wv", wv, send_k, HD)
    for peer in kv_peers:
        to_owner(10, send_k, recv_k, peer)
    own_to_owner(10, send_k, recv_k)

    lane = lax.broadcasted_iota(jnp.int32, (NEW, 128), 1)

    @pl.when(is_owner)
    def _():
        for group in (1, 0):
            arrived_at_owner(0, recv_a, group)
            total = recv_a[group, 0].astype(F32)
            own_bias = total[:, HD:]
            for j in range(1, KV):
                total = total + recv_a[group, j].astype(F32)
            inv_norm = lax.rsqrt(total[:, 2 * HD - 1 : 2 * HD] / D + EPSILON)
            query = (inv_norm * total[:, 0:HD]).astype(BF16)
            send_q[group] = query
            to_members(1, send_q, recv_q, group)
            if group:
                recv_q[pl.ds(k, 1)] = query[None]
            forget_lane = 2 * (t - 1 + group) + head
            forget_sum = jnp.sum(
                jnp.where(lane == forget_lane, total[:, HD:], 0.0), axis=1, keepdims=True
            )
            of_head = (lane >= 16) & (lane < 22) & (lax.rem(lane, 2) == head)
            gate_bias = jnp.sum(jnp.where(of_head, own_bias, 0.0), axis=1, keepdims=True)
            gate_in = inv_norm * forget_sum + gate_bias
            log_forget = jnp.minimum(gate_in, 0.0) - jnp.log1p(jnp.exp(-jnp.abs(gate_in)))
            state[group, :, 0:HD] = query.astype(F32)
            state[group, :, 3 * HD : 4 * HD] = jnp.broadcast_to(log_forget, (NEW, HD))
            state[group, :, 4 * HD :] = jnp.broadcast_to(inv_norm, (NEW, HD))

    arrived_at_member(1, recv_q)
    for s in range(SEQS):
        for h in range(HEADS):
            qblk[s, NEW * h : NEW * h + NEW, HD * h : HD * h + HD] = recv_q[2 * s + h].astype(F32)
    for dz in (4, 5, 3, 6, 2, 7, 1, 0):
        z_peer = lax.rem(z + dz, ZS)
        for s in (2 * z_peer, 2 * z_peer + 1):
            scores = jnp.dot(qblk[s].astype(BF16), kt[s], preferred_element_type=F32)
            scores = scores * score_scale + bias[s]
            peak = jnp.maximum(jnp.max(scores, axis=1, keepdims=True), PEAK_FLOOR)
            peak = peak.astype(BF16).astype(F32)
            weights = jnp.exp(scores - peak)
            block_total = jnp.sum(weights, axis=1, keepdims=True)
            block_sum = jnp.dot(weights.astype(BF16), vc[s], preferred_element_type=F32)
            high = block_total.astype(BF16).astype(F32)
            stats = jnp.where(
                lane8 == 0,
                peak,
                jnp.where(lane8 == 1, high, jnp.where(lane8 == 2, block_total - high, last[s])),
            )
            for h in range(HEADS):
                lines = slice(NEW * h, NEW * h + NEW)
                send_b[2 * s + h, :, 0:HD] = block_sum[lines, HD * h : HD * h + HD].astype(BF16)
                send_b[2 * s + h, :, HD:] = stats[lines].astype(BF16)
        for dy in (2, 1, 3, 0):
            if dz or dy:
                to_owner(2, send_b, recv_b, z_peer * YS + lax.rem(y + dy, YS))
    own_to_owner(2, send_b, recv_b)

    token = lax.broadcasted_iota(jnp.int32, (NEW, 1), 0)

    @pl.when(is_owner)
    def _():
        for group in (1, 0):
            arrived_at_owner(10, recv_k, group)
            total = recv_k[group, 0].astype(F32)
            for j in range(1, KV):
                total = total + recv_k[group, j].astype(F32)
            state[group, :, HD : 3 * HD] = (
                (state[group, :, 4 * HD : 4 * HD + 1] * total).astype(BF16).astype(F32)
            )
        for group in (1, 0):
            arrived_at_owner(2, recv_b, group)
            past_peak = recv_b[group, 0, :, HD:].astype(F32)
            for j in range(1, KV):
                past_peak = jnp.maximum(past_peak, recv_b[group, j, :, HD:].astype(F32))
            past_peak = past_peak[:, 0:1]
            weighted = jnp.zeros((NEW, HD), F32)
            gates = jnp.zeros((NEW, HD), F32)
            past_sum = jnp.zeros((NEW, HD), F32)
            for j in range(KV):
                stats = recv_b[group, j, :, HD:].astype(F32)
                factor = jnp.exp(stats[:, 0:1] - past_peak)
                weighted = weighted + stats * factor
                gates = gates + stats
                past_sum = past_sum + recv_b[group, j, :, 0:HD].astype(F32) * factor
            past_total = weighted[:, 1:2] + weighted[:, 2:3]
            last_cum = gates[:, 3:4] + gates[:, 4:5] + gates[:, 5:6]
            query_wide = state[group, :, 0:HD]
            key_new = state[group, :, HD : 2 * HD]
            value_new = state[group, :, 2 * HD : 3 * HD]
            log_forget = state[group, :, 3 * HD : 3 * HD + 1]
            key_cum = last_cum[0:1, :]
            own_scores = []
            for i in range(NEW):
                key_cum = key_cum + log_forget[i : i + 1, :]
                dots = jnp.sum(query_wide * key_new[i : i + 1, :], axis=1, keepdims=True)
                own_scores.append(jnp.where(token >= i, dots * score_scale - key_cum, NEG_FILL))
            peak_score = past_peak
            for score in own_scores:
                peak_score = jnp.maximum(peak_score, score)
            past_factor = jnp.exp(past_peak - peak_score)
            numerator = past_sum * past_factor
            denominator = past_total * past_factor
            for i, score in enumerate(own_scores):
                weight = jnp.where(token >= i, jnp.exp(score - peak_score), 0.0)
                numerator = numerator + weight.astype(BF16).astype(F32) * value_new[i : i + 1, :]
                denominator = denominator + weight
            attended = (numerator / denominator).astype(BF16)
            send_t[group] = attended
            to_members(3, send_t, recv_t, group)
            if group:
                recv_t[pl.ds(k, 1)] = attended[None]

    loads["wo"].wait()
    arrived_at_member(3, recv_t)
    for s in range(SEQS):
        for h in range(HEADS):
            att[NEW * s : NEW * s + NEW, HD * h : HD * h + HD] = recv_t[2 * s + h].astype(F32)

    send_c[0] = jnp.dot(att[...].astype(BF16), wo[...], preferred_element_type=F32).astype(BF16)
    to_tp(4, send_c.at[0], recv_c)
    recv_c[pl.ds(t, 1)] = send_c[...]
    for name in ("mlp", "wg", "wu"):
        loads[name].wait()
    arrived_tp(4, recv_c)
    attn_out = recv_c[0].astype(F32)
    for j in range(1, TP):
        attn_out = attn_out + recv_c[j].astype(F32)
    middle = (xs[...] + attn_out).astype(BF16).astype(F32)
    xs[...] = middle
    scaled2 = (middle * mlp[...]).astype(BF16)

    @pl.when(is_owner)
    def _():
        squares = jnp.broadcast_to(jnp.sum(middle * middle, axis=1, keepdims=True), (ROWS, 128))
        rough = squares.astype(BF16).astype(F32)
        both_parts = jnp.where(lane64 < 64, rough, squares - rough)
        for s in range(SEQS):
            piece = both_parts[NEW * s : NEW * s + NEW, :].astype(BF16)
            for half in range(2):
                send_e[2 * s + half, :, 0:128] = piece

    def partial_products(dst, at, begin, width, half):
        for n, w in enumerate((wg, wu)):
            part = jnp.dot(scaled2, w[:, begin : begin + width], preferred_element_type=F32)
            for s in range(SEQS):
                dst[2 * s + half, :, at + width * n : at + width * n + width] = part[
                    NEW * s : NEW * s + NEW
                ].astype(BF16)

    for half in range(2):
        partial_products(send_e, 128, CUT * half, FIRST, half)

    @pl.when(is_owner)
    def _():
        for peer in kv_peers:
            to_owner(5, send_e, recv_e, peer)

    @pl.when(no_owner)
    def _():
        for peer in kv_peers:
            to_owner(5, send_e, recv_e, peer, 2 * FIRST, 128)

    own_to_owner(5, send_e, recv_e, 2 * FIRST, 128)
    for half in range(2):
        partial_products(send_l, 0, CUT * half + FIRST, LATE[half] // 2, half)
    for dz, dy in OFFSETS:
        peer = lax.rem(z + dz, ZS) * YS + lax.rem(y + dy, YS)
        half = lax.rem(y + dy, 2)
        for h in range(2):

            @pl.when(half == h)
            def _():
                to_owner(8, send_l, recv_l, peer, LATE[h])

    for h in range(2):

        @pl.when(head == h)
        def _():
            own_to_owner(8, send_l, recv_l, LATE[h])

    def hidden_of(gate, up, inv_norm2):
        gate = inv_norm2 * gate
        return (gate * jax.nn.sigmoid(gate) * (inv_norm2 * up)).astype(BF16)

    @pl.when(is_owner)
    def _():
        for group in (1, 0):
            if group:
                arrived_at_owner(5, recv_e, 1)
                total = recv_e[1, 0, :, 0:128].astype(F32)
                for j in range(1, KV):
                    total = total + recv_e[1, j, :, 0:128].astype(F32)
                inv_norm2 = lax.rsqrt((total[:, 0:1] + total[:, 127:128]) / D + EPSILON)
            else:
                arrived_at_owner(5, recv_e, 0, 2 * FIRST, 128)
            total = recv_e[group, 0, :, 128:].astype(F32)
            for j in range(1, KV):
                total = total + recv_e[group, j, :, 128:].astype(F32)
            hidden = hidden_of(total[:, 0:FIRST], total[:, FIRST:], inv_norm2)
            send_h[group] = hidden
            to_members(6, send_h, recv_h, group)
            if group:
                recv_h[pl.ds(k, 1)] = hidden[None]
            state[group, :, 0:HD] = jnp.broadcast_to(inv_norm2, (NEW, HD))
        for h in range(2):

            @pl.when(head == h)
            def _():
                width = LATE[h]
                for group in (1, 0):
                    arrived_at_owner(8, recv_l, group, width)
                    total = recv_l[group, 0, :, 0:width].astype(F32)
                    for j in range(1, KV):
                        total = total + recv_l[group, j, :, 0:width].astype(F32)
                    hidden = hidden_of(
                        total[:, 0 : width // 2], total[:, width // 2 :], state[group, :, 0:1]
                    )
                    send_m[group, :, 0 : width // 2] = hidden
                    to_members(9, send_m, recv_m, group, width // 2)
                    if group:
                        recv_m[pl.ds(k, 1), :, 0 : width // 2] = hidden[None]

    loads["wd"].wait()
    arrived_at_member(6, recv_h)
    for s in range(SEQS):
        for h in range(2):
            hid[NEW * s : NEW * s + NEW, CUT * h : CUT * h + FIRST] = recv_h[2 * s + h].astype(F32)

    def all_slabs(counts):
        together = 16 * sum(counts)
        return tuple(
            blocks.at[pl.ds(0, n)] for n in (together, together - counts[0], together - counts[1])
        )

    def by_role(enough, sem, name):
        for role, buffer in zip(
            (no_owner, is_owner & (head == 0), is_owner & (head == 1)), enough, strict=True
        ):

            @pl.when(role)
            def _():
                with jax.named_scope(name):
                    wait_bytes(buffer, sem)

    by_role(
        all_slabs([width // 256 for width in LATE]),
        recv_sem.at[9, 0],
        "recv9",
    )
    for s in range(SEQS):
        for h in range(2):
            begin, width = CUT * h + FIRST, LATE[h] // 2
            hid[NEW * s : NEW * s + NEW, begin : begin + width] = recv_m[
                2 * s + h, :, 0:width
            ].astype(F32)

    send_f[0] = jnp.dot(hid[...].astype(BF16), wd[...], preferred_element_type=F32).astype(BF16)
    to_tp(7, send_f.at[0], recv_f)
    recv_f[pl.ds(t, 1)] = send_f[...]
    arrived_tp(7, recv_f)
    mixed = recv_f[0].astype(F32)
    for j in range(1, TP):
        mixed = mixed + recv_f[j].astype(F32)
    out_ref[...] = (xs[...] + mixed).astype(BF16)

    for phase, buffer in ((4, recv_c), (7, recv_f)):
        wait_bytes(buffer.at[pl.ds(0, TP - 1)], send_sem.at[phase, 0])
    for group, role in ((0, no_owner), (1, is_owner)):

        @pl.when(role)
        def _():
            for phase, buffer in ((0, recv_a), (2, recv_b), (10, recv_k)):
                wait_bytes(buffer.at[0, pl.ds(0, KV - group)], send_sem.at[phase, 0])
            first = 128 * (1 - group)
            some = recv_e.at[0, pl.ds(0, KV - group), :, pl.ds(first, EARLY - first)]
            wait_bytes(some, send_sem.at[5, 0])

    by_role(
        all_slabs([width // 128 for width in LATE]),
        send_sem.at[8, 0],
        "sent8",
    )

    @pl.when(is_owner)
    def _():
        for group in range(2):
            for phase, buffer in ((1, recv_q), (3, recv_t), (6, recv_h)):
                wait_bytes(buffer.at[pl.ds(0, KV - group)], send_sem.at[phase, group])
        for h in range(2):

            @pl.when(head == h)
            def _():
                for group in range(2):
                    some = recv_m.at[pl.ds(0, KV - group), :, pl.ds(0, LATE[h] // 2)]
                    wait_bytes(some, send_sem.at[9, group])


def on_device(
    tokens,
    mix_gain,
    w_query,
    w_key,
    w_value,
    w_forget,
    forget_bias,
    key_cache,
    value_cache,
    cum_gate,
    lengths,
    w_out,
    mlp_gain,
    w_gate,
    w_up,
    w_down,
):
    in_vmem = [
        tokens,
        mix_gain.reshape(1, WIDTH),
        w_query,
        w_key,
        w_value,
        w_forget.T,
        key_cache,
        value_cache,
        cum_gate,
        w_out,
        mlp_gain.reshape(1, WIDTH),
        w_gate,
        w_up,
        w_down,
    ]
    shapes = [pltpu.VMEM(a.shape, a.dtype) for a in in_vmem]
    shapes[5] = pltpu.VMEM((16, WIDTH), BF16)
    out = pl.pallas_call(
        kernel,
        out_shape=pltpu.VMEM((ROWS, WIDTH), BF16),
        in_specs=[pl.BlockSpec(memory_space=pltpu.HBM)] * (2 + len(in_vmem)),
        out_specs=pl.BlockSpec(memory_space=pltpu.VMEM),
        scratch_shapes=[
            pltpu.SMEM(lengths.shape, lengths.dtype),
            pltpu.SMEM(forget_bias.shape, forget_bias.dtype),
        ]
        + shapes
        + [
            pltpu.VMEM((ROWS, WIDTH), F32),
            pltpu.VMEM((ROWS, 128), F32),
            pltpu.VMEM((SEQS, 8, 2 * HD), F32),
            pltpu.VMEM((SEQS, 2*HD, POS), BF16),
            pltpu.VMEM((SEQS, 8, POS), F32),
            pltpu.VMEM((SEQS, 8, 128), F32),
            pltpu.VMEM((ROWS, 2 * HD), F32),
            pltpu.VMEM((ROWS, FF), F32),
            pltpu.VMEM((2, NEW, 5 * HD), F32),
            pltpu.VMEM((sum(LATE) // 8, NEW, HD), BF16),
            pltpu.VMEM((KV, NEW, 2 * HD), BF16),
            pltpu.VMEM((2, KV, NEW, 2 * HD), BF16),
            pltpu.VMEM((KV, NEW, 2 * HD), BF16),
            pltpu.VMEM((2, KV, NEW, 2 * HD), BF16),
            pltpu.VMEM((2, NEW, HD), BF16),
            pltpu.VMEM((KV, NEW, HD), BF16),
            pltpu.VMEM((KV, NEW, 2 * HD), BF16),
            pltpu.VMEM((2, KV, NEW, 2 * HD), BF16),
            pltpu.VMEM((2, NEW, HD), BF16),
            pltpu.VMEM((KV, NEW, HD), BF16),
            pltpu.VMEM((1, ROWS, WIDTH), BF16),
            pltpu.VMEM((TP, ROWS, WIDTH), BF16),
            pltpu.VMEM((KV, NEW, EARLY), BF16),
            pltpu.VMEM((2, KV, NEW, EARLY), BF16),
            pltpu.VMEM((KV, NEW, LATE[0]), BF16),
            pltpu.VMEM((2, KV, NEW, LATE[0]), BF16),
            pltpu.VMEM((2, NEW, FIRST), BF16),
            pltpu.VMEM((KV, NEW, FIRST), BF16),
            pltpu.VMEM((2, NEW, LATE[0] // 2), BF16),
            pltpu.VMEM((KV, NEW, LATE[0] // 2), BF16),
            pltpu.VMEM((1, ROWS, WIDTH), BF16),
            pltpu.VMEM((TP, ROWS, WIDTH), BF16),
            pltpu.SemaphoreType.DMA((2 + len(in_vmem),)),
            pltpu.SemaphoreType.DMA((11, 2)),
            pltpu.SemaphoreType.DMA((11, 2)),
        ],
        compiler_params=pltpu.CompilerParams(
            collective_id=0, has_side_effects=True, vmem_limit_bytes=67043328 - 32768
        ),
    )(lengths, forget_bias, *in_vmem)
    return out.reshape(SEQS, NEW, WIDTH)


def solution(mesh):
    return jax.shard_map(
        on_device,
        mesh=mesh,
        in_specs=(
            P(None, None, "kv"),
            P("kv"),
            P("kv", "tp"),
            P("kv", "tp"),
            P("kv", "tp"),
            P(),
            P("tp"),
            P(None, "kv", "tp"),
            P(None, "kv", "tp"),
            P(None, "tp", "kv"),
            P(),
            P("tp", "kv"),
            P("kv"),
            P("kv", "tp"),
            P("kv", "tp"),
            P("tp", "kv"),
        ),
        out_specs=P(None, None, "kv"),
        check_vma=False,
    )
```

```python
import jax
import jax.numpy as jnp
from jax import lax
from jax.experimental import pallas as pl
from jax.experimental.pallas import tpu as pltpu
from jax.sharding import PartitionSpec as P

D = 4096
EPSILON = 1e-06
NEG_FILL = -1e30
PEAK_FLOOR = -1e29
SEQS = 16
NEW = 4
ROWS = SEQS * NEW
HEADS = 2
HD = 128
WIDTH = 128
POS = 512
FF = 1408
CUT = 768
FIRST = 384
EARLY = 128 + 2 * FIRST
LATE = (2 * (CUT - FIRST), 2 * (FF - CUT - FIRST))
KV = 32
TP = 8
ZS, YS = 8, 4
F32 = jnp.float32
BF16 = jnp.bfloat16
MESH = pl.DeviceIdType.MESH


OFFSETS = sorted(
    ((dz, dy) for dz in range(ZS) for dy in range(YS) if dz or dy),
    key=lambda o: -(min(o[0], ZS - o[0]) + min(o[1], YS - o[1])),
)


def kernel(
    lengths_hbm,
    bias_hbm,
    tokens_hbm,
    mix_hbm,
    wq_hbm,
    wk_hbm,
    wv_hbm,
    wf_hbm,
    kc_hbm,
    vc_hbm,
    cg_hbm,
    wo_hbm,
    mlp_hbm,
    wg_hbm,
    wu_hbm,
    wd_hbm,
    out_ref,
    lengths_ref,
    bias_ref,
    tok,
    mix,
    wq,
    wk,
    wv,
    wf,
    kc,
    vc,
    cg,
    wo,
    mlp,
    wg,
    wu,
    wd,
    xs,
    est,
    qblk,
    kt,
    bias,
    last,
    att,
    hid,
    state,
    blocks,
    send_a,
    recv_a,
    send_k,
    recv_k,
    send_q,
    recv_q,
    send_b,
    recv_b,
    send_t,
    recv_t,
    send_c,
    recv_c,
    send_e,
    recv_e,
    send_l,
    recv_l,
    send_h,
    recv_h,
    send_m,
    recv_m,
    send_f,
    recv_f,
    in_sem,
    send_sem,
    recv_sem,
):
    k = lax.axis_index("kv")
    t = lax.axis_index("tp")
    z, y = k // YS, lax.rem(k, YS)
    head = lax.rem(k, 2)
    mine = k // 2

    loads = {}
    sources = dict(
        tok=(tokens_hbm, tok),
        mix=(mix_hbm, mix),
        bias=(bias_hbm, bias_ref),
        wq=(wq_hbm, wq),
        wf=(wf_hbm.at[:, pl.ds(pl.multiple_of(k * WIDTH, WIDTH), WIDTH)], wf),
        lengths=(lengths_hbm, lengths_ref),
        wk=(wk_hbm, wk),
        wv=(wv_hbm, wv),
        kc=(kc_hbm, kc),
        vc=(vc_hbm, vc),
        cg=(cg_hbm, cg),
        wo=(wo_hbm, wo),
        mlp=(mlp_hbm, mlp),
        wg=(wg_hbm, wg),
        wu=(wu_hbm, wu),
        wd=(wd_hbm, wd),
    )
    kv_peers = [lax.rem(z + dz, ZS) * YS + lax.rem(y + dy, YS) for dz, dy in OFFSETS]
    tp_peers = [lax.rem(t + d, TP) for d in (4, 5, 3, 2, 6, 7, 1)]
    core = lax.rem(t, 2)
    owner_t = t + 1 - core
    is_owner = core == 1
    no_owner = core == 0

    barrier = pltpu.get_barrier_semaphore()

    for n, (name, (src, dst)) in enumerate(sources.items()):
        loads[name] = pltpu.make_async_copy(src, dst, in_sem.at[n])
    for name in list(sources)[:5]:
        loads[name].start()

    def greet(kv, tp):
        pl.semaphore_signal(barrier, inc=1, device_id=(kv, tp), device_id_type=MESH)

    for peer in kv_peers:
        greet(peer, owner_t)

    @pl.when(is_owner)
    def _():
        for peer in kv_peers:
            greet(peer, t - 1)

    for peer in tp_peers:
        greet(k, peer)

    for name in list(sources)[5:]:
        loads[name].start()

    def send(src, dst, sent, received, kv, tp):
        pltpu.make_async_remote_copy(
            src_ref=src,
            dst_ref=dst,
            send_sem=sent,
            recv_sem=received,
            device_id=(kv, tp),
            device_id_type=MESH,
        ).start()

    def lanes(ref, width, begin=0):
        return ref if width is None else ref.at[:, pl.ds(begin, width)]

    def to_owner(phase, src, dst, peer, width=None, begin=0):
        send(
            lanes(src.at[peer], width, begin),
            lanes(dst.at[core, k], width, begin),
            send_sem.at[phase, 0],
            recv_sem.at[phase, core],
            peer,
            owner_t,
        )

    def own_to_owner(phase, src, dst, width=None, begin=0):
        @pl.when(no_owner)
        def _():
            to_owner(phase, src, dst, k, width, begin)

        @pl.when(is_owner)
        def _():
            dst[1, pl.ds(k, 1)] = src[pl.ds(k, 1)]

    def to_members(phase, src, dst, group, width=None):
        peers = kv_peers if group else kv_peers + [k]
        for peer in peers:
            send(
                lanes(src.at[group], width),
                lanes(dst.at[k], width),
                send_sem.at[phase, group],
                recv_sem.at[phase, 0],
                peer,
                t - 1 + group,
            )

    def to_tp(phase, src, dst):
        for peer in tp_peers:
            send(src, dst.at[t], send_sem.at[phase, 0], recv_sem.at[phase, 0], k, peer)

    def wait_bytes(ref, sem):
        pltpu.make_async_copy(ref, ref, sem).wait()

    def arrived_at_owner(phase, dst, group, width=None, begin=0):
        count = KV - group
        some = dst.at[group, pl.ds(0, count)]
        if width is not None:
            some = dst.at[group, pl.ds(0, count), :, pl.ds(begin, width)]
        with jax.named_scope("own%d_%d" % (phase, group)):
            wait_bytes(some, recv_sem.at[phase, group])

    def arrived_at_member(phase, dst):
        for group, role in ((0, no_owner), (1, is_owner)):

            @pl.when(role)
            def _():
                with jax.named_scope("recv%d" % phase):
                    wait_bytes(dst.at[pl.ds(0, KV - group)], recv_sem.at[phase, 0])

    def arrived_tp(phase, dst):
        with jax.named_scope("recv%d" % phase):
            wait_bytes(dst.at[pl.ds(0, TP - 1)], recv_sem.at[phase, 0])

    for name in ("tok", "mix"):
        loads[name].wait()
    for s in range(SEQS):
        xs[NEW * s : NEW * s + NEW, :] = tok[s].astype(F32)
    x = xs[...]
    scaled = (x * mix[...]).astype(BF16)
    est[...] = jnp.broadcast_to(jnp.sum(x * x, axis=1, keepdims=True), (ROWS, 128))
    loads["wf"].wait()
    est[:, 0:16] = lax.dot_general(
        scaled, wf[...], (((1,), (1,)), ((), ())), preferred_element_type=F32
    )
    loads["bias"].wait()
    lane64 = lax.broadcasted_iota(jnp.int32, (ROWS, 128), 1)
    bias_all = jnp.where(lax.rem(lane64, 2) == 0, bias_ref[0], bias_ref[1])
    high = bias_all.astype(BF16).astype(F32)
    middle_part = (bias_all - high).astype(BF16).astype(F32)
    low = bias_all - high - middle_part
    parts = jnp.where(lane64 < 18, high, jnp.where(lane64 < 20, middle_part, low))
    est[...] = jnp.where((lane64 >= 16) & (lane64 < 22), parts, est[...])
    def project(name, w, dst, at):
        loads[name].wait()
        part = jnp.dot(scaled, w[...], preferred_element_type=F32)
        for s in range(SEQS):
            for h in range(HEADS):
                dst[2 * s + h, :, at : at + HD] = part[
                    NEW * s : NEW * s + NEW, HD * h : HD * h + HD
                ].astype(BF16)

    project("wq", wq, send_a, 0)
    for s in range(SEQS):
        piece = est[NEW * s : NEW * s + NEW, :].astype(BF16)
        for h in range(HEADS):
            send_a[2 * s + h, :, HD:] = piece
    with jax.named_scope("barrier"):
        pl.semaphore_wait(barrier, KV - 1 + TP - 1 + (KV - 1) * core)
    for peer in kv_peers:
        to_owner(0, send_a, recv_a, peer)
    own_to_owner(0, send_a, recv_a)

    qblk[...] = jnp.zeros(qblk.shape, F32)
    for name in ("kc", "vc", "cg", "lengths"):
        loads[name].wait()
    score_scale = HD**-0.5
    position = k * POS + lax.broadcasted_iota(jnp.int32, (8, POS), 1)
    row8 = lax.broadcasted_iota(jnp.int32, (8, POS), 0)
    lane8 = lax.broadcasted_iota(jnp.int32, (8, 128), 1)
    for s in range(SEQS):
        length = lengths_ref[s]
        both = cg[s]
        cum = jnp.where(row8 < NEW, both[0:1, :], both[1:2, :])
        bias[s] = jnp.where(position < length, -cum, NEG_FILL)
        at_last = jnp.sum(jnp.where(position == length - 1, cum, 0.0), axis=1, keepdims=True)
        high = at_last.astype(BF16).astype(F32)
        middle_part = (at_last - high).astype(BF16).astype(F32)
        low = at_last - high - middle_part
        last[s] = jnp.where(
            lane8 == 3, high, jnp.where(lane8 == 4, middle_part, jnp.where(lane8 == 5, low, 0.0))
        )
    for s in range(SEQS):
        kt[s] = kc[s].T
    project("wk", wk, send_k, 0)
    project("wv", wv, send_k, HD)
    for peer in kv_peers:
        to_owner(10, send_k, recv_k, peer)
    own_to_owner(10, send_k, recv_k)

    lane = lax.broadcasted_iota(jnp.int32, (NEW, 128), 1)

    @pl.when(is_owner)
    def _():
        for group in (1, 0):
            arrived_at_owner(0, recv_a, group)
            total = recv_a[group, 0].astype(F32)
            own_bias = total[:, HD:]
            for j in range(1, KV):
                total = total + recv_a[group, j].astype(F32)
            inv_norm = lax.rsqrt(total[:, 2 * HD - 1 : 2 * HD] / D + EPSILON)
            query = (inv_norm * total[:, 0:HD]).astype(BF16)
            send_q[group] = query
            to_members(1, send_q, recv_q, group)
            if group:
                recv_q[pl.ds(k, 1)] = query[None]
            forget_lane = 2 * (t - 1 + group) + head
            forget_sum = jnp.sum(
                jnp.where(lane == forget_lane, total[:, HD:], 0.0), axis=1, keepdims=True
            )
            of_head = (lane >= 16) & (lane < 22) & (lax.rem(lane, 2) == head)
            gate_bias = jnp.sum(jnp.where(of_head, own_bias, 0.0), axis=1, keepdims=True)
            gate_in = inv_norm * forget_sum + gate_bias
            log_forget = jnp.minimum(gate_in, 0.0) - jnp.log1p(jnp.exp(-jnp.abs(gate_in)))
            state[group, :, 0:HD] = query.astype(F32)
            state[group, :, 3 * HD : 4 * HD] = jnp.broadcast_to(log_forget, (NEW, HD))
            state[group, :, 4 * HD :] = jnp.broadcast_to(inv_norm, (NEW, HD))

    arrived_at_member(1, recv_q)
    for s in range(SEQS):
        for h in range(HEADS):
            qblk[s, NEW * h : NEW * h + NEW, HD * h : HD * h + HD] = recv_q[2 * s + h].astype(F32)
    for dz in (4, 5, 3, 6, 2, 7, 1, 0):
        z_peer = lax.rem(z + dz, ZS)
        for s in (2 * z_peer, 2 * z_peer + 1):
            scores = jnp.dot(qblk[s].astype(BF16), kt[s], preferred_element_type=F32)
            scores = scores * score_scale + bias[s]
            peak = jnp.maximum(jnp.max(scores, axis=1, keepdims=True), PEAK_FLOOR)
            peak = peak.astype(BF16).astype(F32)
            weights = jnp.exp(scores - peak)
            block_total = jnp.sum(weights, axis=1, keepdims=True)
            block_sum = jnp.dot(weights.astype(BF16), vc[s], preferred_element_type=F32)
            high = block_total.astype(BF16).astype(F32)
            stats = jnp.where(
                lane8 == 0,
                peak,
                jnp.where(lane8 == 1, high, jnp.where(lane8 == 2, block_total - high, last[s])),
            )
            for h in range(HEADS):
                lines = slice(NEW * h, NEW * h + NEW)
                send_b[2 * s + h, :, 0:HD] = block_sum[lines, HD * h : HD * h + HD].astype(BF16)
                send_b[2 * s + h, :, HD:] = stats[lines].astype(BF16)
        for dy in (2, 1, 3, 0):
            if dz or dy:
                to_owner(2, send_b, recv_b, z_peer * YS + lax.rem(y + dy, YS))
    own_to_owner(2, send_b, recv_b)

    token = lax.broadcasted_iota(jnp.int32, (NEW, 1), 0)

    @pl.when(is_owner)
    def _():
        for group in (1, 0):
            arrived_at_owner(10, recv_k, group)
            total = recv_k[group, 0].astype(F32)
            for j in range(1, KV):
                total = total + recv_k[group, j].astype(F32)
            state[group, :, HD : 3 * HD] = (
                (state[group, :, 4 * HD : 4 * HD + 1] * total).astype(BF16).astype(F32)
            )
        for group in (1, 0):
            arrived_at_owner(2, recv_b, group)
            stats = recv_b[group, :, :, HD:].astype(F32)
            past_peak = jnp.max(stats, axis=0)[:, 0:1]
            factor = jnp.exp(stats[:, :, 0:1] - past_peak[None])
            weighted = jnp.sum(stats * factor, axis=0)
            gates = jnp.sum(stats, axis=0)
            past_sum = jnp.sum(recv_b[group, :, :, 0:HD].astype(F32) * factor, axis=0)
            past_total = weighted[:, 1:2] + weighted[:, 2:3]
            last_cum = gates[:, 3:4] + gates[:, 4:5] + gates[:, 5:6]
            query_wide = state[group, :, 0:HD]
            key_new = state[group, :, HD : 2 * HD]
            value_new = state[group, :, 2 * HD : 3 * HD]
            log_forget = state[group, :, 3 * HD : 3 * HD + 1]
            key_cum = last_cum[0:1, :]
            own_scores = []
            for i in range(NEW):
                key_cum = key_cum + log_forget[i : i + 1, :]
                dots = jnp.sum(query_wide * key_new[i : i + 1, :], axis=1, keepdims=True)
                own_scores.append(jnp.where(token >= i, dots * score_scale - key_cum, NEG_FILL))
            peak_score = past_peak
            for score in own_scores:
                peak_score = jnp.maximum(peak_score, score)
            past_factor = jnp.exp(past_peak - peak_score)
            numerator = past_sum * past_factor
            denominator = past_total * past_factor
            for i, score in enumerate(own_scores):
                weight = jnp.where(token >= i, jnp.exp(score - peak_score), 0.0)
                numerator = numerator + weight.astype(BF16).astype(F32) * value_new[i : i + 1, :]
                denominator = denominator + weight
            attended = (numerator / denominator).astype(BF16)
            send_t[group] = attended
            to_members(3, send_t, recv_t, group)
            if group:
                recv_t[pl.ds(k, 1)] = attended[None]

    loads["wo"].wait()
    arrived_at_member(3, recv_t)
    for s in range(SEQS):
        for h in range(HEADS):
            att[NEW * s : NEW * s + NEW, HD * h : HD * h + HD] = recv_t[2 * s + h].astype(F32)

    send_c[0] = jnp.dot(att[...].astype(BF16), wo[...], preferred_element_type=F32).astype(BF16)
    to_tp(4, send_c.at[0], recv_c)
    recv_c[pl.ds(t, 1)] = send_c[...]
    for name in ("mlp", "wg", "wu"):
        loads[name].wait()
    arrived_tp(4, recv_c)
    attn_out = recv_c[0].astype(F32)
    for j in range(1, TP):
        attn_out = attn_out + recv_c[j].astype(F32)
    middle = (xs[...] + attn_out).astype(BF16).astype(F32)
    xs[...] = middle
    scaled2 = (middle * mlp[...]).astype(BF16)

    @pl.when(is_owner)
    def _():
        squares = jnp.broadcast_to(jnp.sum(middle * middle, axis=1, keepdims=True), (ROWS, 128))
        rough = squares.astype(BF16).astype(F32)
        both_parts = jnp.where(lane64 < 64, rough, squares - rough)
        for s in range(SEQS):
            piece = both_parts[NEW * s : NEW * s + NEW, :].astype(BF16)
            for half in range(2):
                send_e[2 * s + half, :, 0:128] = piece

    def partial_products(dst, at, begin, width, half):
        for n, w in enumerate((wg, wu)):
            part = jnp.dot(scaled2, w[:, begin : begin + width], preferred_element_type=F32)
            for s in range(SEQS):
                dst[2 * s + half, :, at + width * n : at + width * n + width] = part[
                    NEW * s : NEW * s + NEW
                ].astype(BF16)

    for half in range(2):
        partial_products(send_e, 128, CUT * half, FIRST, half)

    @pl.when(is_owner)
    def _():
        for peer in kv_peers:
            to_owner(5, send_e, recv_e, peer)

    @pl.when(no_owner)
    def _():
        for peer in kv_peers:
            to_owner(5, send_e, recv_e, peer, 2 * FIRST, 128)

    own_to_owner(5, send_e, recv_e, 2 * FIRST, 128)
    for half in range(2):
        partial_products(send_l, 0, CUT * half + FIRST, LATE[half] // 2, half)
    for dz, dy in OFFSETS:
        peer = lax.rem(z + dz, ZS) * YS + lax.rem(y + dy, YS)
        half = lax.rem(y + dy, 2)
        for h in range(2):

            @pl.when(half == h)
            def _():
                to_owner(8, send_l, recv_l, peer, LATE[h])

    for h in range(2):

        @pl.when(head == h)
        def _():
            own_to_owner(8, send_l, recv_l, LATE[h])

    def hidden_of(gate, up, inv_norm2):
        gate = inv_norm2 * gate
        return (gate * jax.nn.sigmoid(gate) * (inv_norm2 * up)).astype(BF16)

    @pl.when(is_owner)
    def _():
        for group in (1, 0):
            if group:
                arrived_at_owner(5, recv_e, 1)
                total = recv_e[1, 0, :, 0:128].astype(F32)
                for j in range(1, KV):
                    total = total + recv_e[1, j, :, 0:128].astype(F32)
                inv_norm2 = lax.rsqrt((total[:, 0:1] + total[:, 127:128]) / D + EPSILON)
            else:
                arrived_at_owner(5, recv_e, 0, 2 * FIRST, 128)
            total = recv_e[group, 0, :, 128:].astype(F32)
            for j in range(1, KV):
                total = total + recv_e[group, j, :, 128:].astype(F32)
            hidden = hidden_of(total[:, 0:FIRST], total[:, FIRST:], inv_norm2)
            send_h[group] = hidden
            to_members(6, send_h, recv_h, group)
            if group:
                recv_h[pl.ds(k, 1)] = hidden[None]
            state[group, :, 0:HD] = jnp.broadcast_to(inv_norm2, (NEW, HD))
        for h in range(2):

            @pl.when(head == h)
            def _():
                width = LATE[h]
                for group in (1, 0):
                    arrived_at_owner(8, recv_l, group, width)
                    total = recv_l[group, 0, :, 0:width].astype(F32)
                    for j in range(1, KV):
                        total = total + recv_l[group, j, :, 0:width].astype(F32)
                    hidden = hidden_of(
                        total[:, 0 : width // 2], total[:, width // 2 :], state[group, :, 0:1]
                    )
                    send_m[group, :, 0 : width // 2] = hidden
                    to_members(9, send_m, recv_m, group, width // 2)
                    if group:
                        recv_m[pl.ds(k, 1), :, 0 : width // 2] = hidden[None]

    loads["wd"].wait()
    arrived_at_member(6, recv_h)
    for s in range(SEQS):
        for h in range(2):
            hid[NEW * s : NEW * s + NEW, CUT * h : CUT * h + FIRST] = recv_h[2 * s + h].astype(F32)

    def all_slabs(counts):
        together = 16 * sum(counts)
        return tuple(
            blocks.at[pl.ds(0, n)] for n in (together, together - counts[0], together - counts[1])
        )

    def by_role(enough, sem, name):
        for role, buffer in zip(
            (no_owner, is_owner & (head == 0), is_owner & (head == 1)), enough, strict=True
        ):

            @pl.when(role)
            def _():
                with jax.named_scope(name):
                    wait_bytes(buffer, sem)

    by_role(
        all_slabs([width // 256 for width in LATE]),
        recv_sem.at[9, 0],
        "recv9",
    )
    for s in range(SEQS):
        for h in range(2):
            begin, width = CUT * h + FIRST, LATE[h] // 2
            hid[NEW * s : NEW * s + NEW, begin : begin + width] = recv_m[
                2 * s + h, :, 0:width
            ].astype(F32)

    send_f[0] = jnp.dot(hid[...].astype(BF16), wd[...], preferred_element_type=F32).astype(BF16)
    to_tp(7, send_f.at[0], recv_f)
    recv_f[pl.ds(t, 1)] = send_f[...]
    arrived_tp(7, recv_f)
    mixed = recv_f[0].astype(F32)
    for j in range(1, TP):
        mixed = mixed + recv_f[j].astype(F32)
    out_ref[...] = (xs[...] + mixed).astype(BF16)

    for phase, buffer in ((4, recv_c), (7, recv_f)):
        wait_bytes(buffer.at[pl.ds(0, TP - 1)], send_sem.at[phase, 0])
    for group, role in ((0, no_owner), (1, is_owner)):

        @pl.when(role)
        def _():
            for phase, buffer in ((0, recv_a), (2, recv_b), (10, recv_k)):
                wait_bytes(buffer.at[0, pl.ds(0, KV - group)], send_sem.at[phase, 0])
            first = 128 * (1 - group)
            some = recv_e.at[0, pl.ds(0, KV - group), :, pl.ds(first, EARLY - first)]
            wait_bytes(some, send_sem.at[5, 0])

    by_role(
        all_slabs([width // 128 for width in LATE]),
        send_sem.at[8, 0],
        "sent8",
    )

    @pl.when(is_owner)
    def _():
        for group in range(2):
            for phase, buffer in ((1, recv_q), (3, recv_t), (6, recv_h)):
                wait_bytes(buffer.at[pl.ds(0, KV - group)], send_sem.at[phase, group])
        for h in range(2):

            @pl.when(head == h)
            def _():
                for group in range(2):
                    some = recv_m.at[pl.ds(0, KV - group), :, pl.ds(0, LATE[h] // 2)]
                    wait_bytes(some, send_sem.at[9, group])


def on_device(
    tokens,
    mix_gain,
    w_query,
    w_key,
    w_value,
    w_forget,
    forget_bias,
    key_cache,
    value_cache,
    cum_gate,
    lengths,
    w_out,
    mlp_gain,
    w_gate,
    w_up,
    w_down,
):
    in_vmem = [
        tokens,
        mix_gain.reshape(1, WIDTH),
        w_query,
        w_key,
        w_value,
        w_forget.T,
        key_cache,
        value_cache,
        cum_gate,
        w_out,
        mlp_gain.reshape(1, WIDTH),
        w_gate,
        w_up,
        w_down,
    ]
    shapes = [pltpu.VMEM(a.shape, a.dtype) for a in in_vmem]
    shapes[5] = pltpu.VMEM((16, WIDTH), BF16)
    out = pl.pallas_call(
        kernel,
        out_shape=pltpu.VMEM((ROWS, WIDTH), BF16),
        in_specs=[pl.BlockSpec(memory_space=pltpu.HBM)] * (2 + len(in_vmem)),
        out_specs=pl.BlockSpec(memory_space=pltpu.VMEM),
        scratch_shapes=[
            pltpu.SMEM(lengths.shape, lengths.dtype),
            pltpu.SMEM(forget_bias.shape, forget_bias.dtype),
        ]
        + shapes
        + [
            pltpu.VMEM((ROWS, WIDTH), F32),
            pltpu.VMEM((ROWS, 128), F32),
            pltpu.VMEM((SEQS, 8, 2 * HD), F32),
            pltpu.VMEM((SEQS, 2*HD, POS), BF16),
            pltpu.VMEM((SEQS, 8, POS), F32),
            pltpu.VMEM((SEQS, 8, 128), F32),
            pltpu.VMEM((ROWS, 2 * HD), F32),
            pltpu.VMEM((ROWS, FF), F32),
            pltpu.VMEM((2, NEW, 5 * HD), F32),
            pltpu.VMEM((sum(LATE) // 8, NEW, HD), BF16),
            pltpu.VMEM((KV, NEW, 2 * HD), BF16),
            pltpu.VMEM((2, KV, NEW, 2 * HD), BF16),
            pltpu.VMEM((KV, NEW, 2 * HD), BF16),
            pltpu.VMEM((2, KV, NEW, 2 * HD), BF16),
            pltpu.VMEM((2, NEW, HD), BF16),
            pltpu.VMEM((KV, NEW, HD), BF16),
            pltpu.VMEM((KV, NEW, 2 * HD), BF16),
            pltpu.VMEM((2, KV, NEW, 2 * HD), BF16),
            pltpu.VMEM((2, NEW, HD), BF16),
            pltpu.VMEM((KV, NEW, HD), BF16),
            pltpu.VMEM((1, ROWS, WIDTH), BF16),
            pltpu.VMEM((TP, ROWS, WIDTH), BF16),
            pltpu.VMEM((KV, NEW, EARLY), BF16),
            pltpu.VMEM((2, KV, NEW, EARLY), BF16),
            pltpu.VMEM((KV, NEW, LATE[0]), BF16),
            pltpu.VMEM((2, KV, NEW, LATE[0]), BF16),
            pltpu.VMEM((2, NEW, FIRST), BF16),
            pltpu.VMEM((KV, NEW, FIRST), BF16),
            pltpu.VMEM((2, NEW, LATE[0] // 2), BF16),
            pltpu.VMEM((KV, NEW, LATE[0] // 2), BF16),
            pltpu.VMEM((1, ROWS, WIDTH), BF16),
            pltpu.VMEM((TP, ROWS, WIDTH), BF16),
            pltpu.SemaphoreType.DMA((2 + len(in_vmem),)),
            pltpu.SemaphoreType.DMA((11, 2)),
            pltpu.SemaphoreType.DMA((11, 2)),
        ],
        compiler_params=pltpu.CompilerParams(
            collective_id=0, has_side_effects=True, vmem_limit_bytes=67043328 - 32768
        ),
    )(lengths, forget_bias, *in_vmem)
    return out.reshape(SEQS, NEW, WIDTH)


def solution(mesh):
    return jax.shard_map(
        on_device,
        mesh=mesh,
        in_specs=(
            P(None, None, "kv"),
            P("kv"),
            P("kv", "tp"),
            P("kv", "tp"),
            P("kv", "tp"),
            P(),
            P("tp"),
            P(None, "kv", "tp"),
            P(None, "kv", "tp"),
            P(None, "tp", "kv"),
            P(),
            P("tp", "kv"),
            P("kv"),
            P("kv", "tp"),
            P("kv", "tp"),
            P("tp", "kv"),
        ),
        out_specs=P(None, None, "kv"),
        check_vma=False,
    )
```
